128 devices in a mesh: sp: 16 (over z, y), tp: 8 (over x, core).
Axes of the slice: x: 4, y: 4, z: 4, core: 2. Of those that a mesh axis runs over, the one named last changes fastest.
Arguments:
- queries: bfloat16 [16384, 1024], P('sp', 'tp'), may hold values from -8 to 8
- keyvals: bfloat16 [16384, 8, 128], P('sp', 'tp'), may hold values from -8 to 8
- head_sink_logit: float32 [16], P('tp'), may hold values from 2 to 7
- doc_ids: int32 [16384], P('sp'), may hold values from 0 to 7, never falling along the last dimension, each value on 1 to 4096 neighbouring positions
- stream_in: bfloat16 [16384, 2048], P(('sp', 'tp')), may hold values from -6 to 6
- out_weight: bfloat16 [1024, 2048], replicated, may hold values from -1.5 to 1.5
- first_gain: float32 [2048], replicated, may hold values from 0.1 to 1.9
- up_weight: bfloat16 [2048, 8192], P('sp', 'tp'), may hold values from -0.125 to 0.125
- down_weight: bfloat16 [8192, 2048], P('tp', 'sp'), may hold values from -0.0625 to 0.0625
- second_gain: float32 [2048], replicated, may hold values from 0.1 to 1.9
Outputs:
- layer_out: bfloat16 [16384, 2048], P(('sp', 'tp'))
The draws below stay inside these ranges and needn't reach their ends.
Inputs may be any that keep to these rules, and one draw needn't show every extreme that they name: `doc_ids`: document numbers never fall along the sequence.
All inputs are finite; a program needn't handle non-finite values.
Results may differ from the reference program's by a relative error of at most 0.013.
Values may be sent and summed in bfloat16 or wider, within the bound.
A program may use at most 64 MiB of HBM per device.

```python
import math
import jax
import jax.numpy as jnp
import numpy as np
from jax import lax

D = 2048
FF = 8192
QUERY_HEADS = 16
KEY_VALUE_HEADS = 8
HEAD_SIZE = 64
WINDOW_REACH = 128
PACKED_TOKENS = 16384
N_SP = 16
N_TP = 8


def draw_queries(key, part):
    self_key = jax.random.fold_in(key, 3)
    value_rows = jnp.clip(jax.random.normal(self_key, (PACKED_TOKENS, QUERY_HEADS, HEAD_SIZE), jnp.float32), -6.0, 6.0)
    return value_rows.reshape(PACKED_TOKENS, QUERY_HEADS * HEAD_SIZE).astype(jnp.bfloat16)


def draw_keyvals(key, part):
    self_key = jax.random.fold_in(key, 5)
    value_rows = jnp.clip(jax.random.normal(self_key, (PACKED_TOKENS, KEY_VALUE_HEADS, 2 * HEAD_SIZE), jnp.float32), -6.0, 6.0)
    return value_rows.astype(jnp.bfloat16)


def levels(stream_key, shape, cuts, smallest, high):
    def one(position, shards_of):
        steps = jax.random.uniform(jax.random.fold_in(jax.random.fold_in(stream_key, 6), position), (shards_of,), jnp.float32, smallest / len(cuts), high / len(cuts))
        return jnp.repeat(jnp.exp(steps), shape[position] // shards_of).reshape((-1,) + (1,) * (len(shape) - position - 1))

    level = one(*cuts[0])
    for cut in cuts[1:]:
        level = level * one(*cut)
    return level


def profile(number_of, total, most, slope):
    weights = [(1 << 20) // math.isqrt(grade ** slope) + 1 for grade in range(2, number_of + 1)]
    spare, given = total - most - (number_of - 1), [1] * (number_of - 1)
    while spare > 0:
        movable = [i for i in range(number_of - 1) if given[i] < most]
        pool, remaining = sum([weights[i] for i in movable]), spare
        for i in movable:
            extra = min(most - given[i], max(1, remaining * weights[i] // pool), spare)
            given[i] = given[i] + extra
            spare = spare - extra
    return np.array([most] + given)


def uneven(rng, count, total, most, skew):
    if count == 2:
        one = jax.random.randint(rng, (), max(1, total - most), min(most, total - 1) + 1)
        return jnp.stack([one, total - one])
    lengths = jnp.asarray(profile(count, total, most, skew), jnp.int32)
    couples = (count - 1) // 2
    source_of, sink = lengths[1:1 + 2 * couples:2], lengths[2:2 + 2 * couples:2]
    margin = jnp.minimum(source_of - 1, most - sink)
    passed = jax.random.randint(jax.random.fold_in(rng, 1), (couples,), 0, 1 << 20) % (margin + 1)
    lengths = lengths.at[1:1 + 2 * couples:2].set(source_of - passed).at[2:2 + 2 * couples:2].set(sink + passed)
    return lengths[jax.random.permutation(jax.random.fold_in(rng, 2), count)]


def noise(stream_key, shape, scale, most, shards=(), kind=jnp.bfloat16):
    array = jax.random.normal(stream_key, shape, jnp.float32) * scale
    if len(shards) > 0:
        array = levels(stream_key, shape, shards, -0.22, 0.18) * array
    return jnp.clip(array, min=-most, max=most).astype(kind)


def setup_inputs(seed: int = 0) -> dict:
    seeds = jax.random.split(jax.random.key(seed), 11)
    queries = draw_queries(jax.random.fold_in(seeds[10], 71), 0)
    keyvals = draw_keyvals(jax.random.fold_in(seeds[10], 71), 0)
    head_sink_logit = jnp.clip(2.0 + 5.0 * jax.random.uniform(seeds[2], (QUERY_HEADS,), jnp.float32) ** levels(seeds[2], (QUERY_HEADS,), ((0, 8),), -0.2, 0.2), 2.0, 7.0)
    doc_ids = jnp.searchsorted(jnp.cumsum(uneven(seeds[3], N_SP // 2, PACKED_TOKENS, PACKED_TOKENS // 4, 1)), jnp.arange(PACKED_TOKENS), side="right").astype(jnp.int32)
    stream_in = noise(seeds[4], (PACKED_TOKENS, D), 1.0, 6.0, ((0, 128),))
    out_weight = noise(seeds[5], (QUERY_HEADS * HEAD_SIZE, D), (QUERY_HEADS * HEAD_SIZE // 64) ** -0.5, 1.5)
    first_gain = jnp.clip(1.0 + 0.18 * jax.random.normal(seeds[6], (D,), jnp.float32), 0.1, 1.9)
    up_weight = noise(seeds[7], (D, FF), D ** -0.5, 0.125, ((0, 16), (1, 8)))
    down_weight = noise(seeds[8], (FF, D), FF ** -0.5, 0.0625, ((0, 8), (1, 16)))
    second_gain = jnp.clip(1.0 + 0.18 * jax.random.normal(seeds[9], (D,), jnp.float32), 0.1, 1.9)
    return dict(queries=queries, keyvals=keyvals, head_sink_logit=head_sink_logit, doc_ids=doc_ids, stream_in=stream_in, out_weight=out_weight, first_gain=first_gain, up_weight=up_weight, down_weight=down_weight, second_gain=second_gain)


NEG_LARGE = -1e+30
NORM_EPS = 1e-05

def layer_norm(stream, gain_row):
    centre = lax.optimization_barrier(jnp.mean(stream, axis=-1, keepdims=True))
    shifted = stream - centre
    spread = lax.optimization_barrier(jnp.mean(shifted * shifted, axis=-1, keepdims=True))
    return shifted * lax.rsqrt(spread + NORM_EPS) * gain_row

def window_attention(queries, keyvals, head_sink_logit, doc_ids):
    block_list = PACKED_TOKENS // WINDOW_REACH
    heads_per_group = QUERY_HEADS // KEY_VALUE_HEADS
    score_scale = HEAD_SIZE ** (-0.5)
    query_block_list = queries.astype(jnp.float32).reshape(block_list, WINDOW_REACH, KEY_VALUE_HEADS, heads_per_group, HEAD_SIZE).transpose(2, 0, 1, 3, 4)
    padding_width = jnp.zeros((WINDOW_REACH, KEY_VALUE_HEADS, 2 * HEAD_SIZE), jnp.float32)
    padded_rows = jnp.concatenate([padding_width, keyvals.astype(jnp.float32), padding_width], axis=0).reshape(block_list + 2, WINDOW_REACH, KEY_VALUE_HEADS, 2 * HEAD_SIZE)
    banded = jnp.concatenate([padded_rows[:-2], padded_rows[1:-1], padded_rows[2:]], axis=1).transpose(2, 0, 1, 3)
    doc_pad = jnp.zeros((WINDOW_REACH,), jnp.int32)
    doc_ext = jnp.concatenate([doc_pad, doc_ids, doc_pad]).reshape(block_list + 2, WINDOW_REACH)
    doc_band = jnp.concatenate([doc_ext[:-2], doc_ext[1:-1], doc_ext[2:]], axis=1)
    query_pos = jnp.arange(PACKED_TOKENS, dtype=jnp.int32).reshape(block_list, WINDOW_REACH, 1)
    key_pos = (jnp.arange(block_list, dtype=jnp.int32)[:, None] * WINDOW_REACH + jnp.arange(3 * WINDOW_REACH, dtype=jnp.int32)[None, :] - WINDOW_REACH)[:, None, :]
    allowed = (jnp.abs(query_pos - key_pos) <= WINDOW_REACH) & (key_pos >= 0) & (key_pos < PACKED_TOKENS) & (doc_ids.reshape(block_list, WINDOW_REACH, 1) == doc_band[:, None, :])
    sink_logit_table = head_sink_logit.reshape(KEY_VALUE_HEADS, heads_per_group)

    def one_head(operands):
        query_head, band_head, sink_head = operands
        scores = jnp.einsum('nqgd,nkd->ngqk', query_head, band_head[..., :HEAD_SIZE]) * score_scale
        scores = jnp.where(allowed[:, None], scores, NEG_LARGE)
        sink_col = sink_head[None, :, None, None]
        highest = jnp.maximum(lax.optimization_barrier(jnp.max(scores, axis=-1, keepdims=True)), sink_col)
        powers = jnp.exp(scores - highest)
        denominator = lax.optimization_barrier(jnp.sum(powers, axis=-1, keepdims=True)) + jnp.exp(sink_col - highest)
        weights = lax.optimization_barrier((powers / denominator).astype(jnp.bfloat16)).astype(jnp.float32)
        mixed_out = jnp.einsum('ngqk,nkd->nqgd', weights, band_head[..., HEAD_SIZE:])
        return mixed_out.astype(jnp.bfloat16)
    heads_out = lax.map(one_head, (query_block_list, banded, sink_logit_table))
    return heads_out.transpose(1, 2, 0, 3, 4).reshape(PACKED_TOKENS, QUERY_HEADS * HEAD_SIZE)

def reference(queries, keyvals, head_sink_logit, doc_ids, stream_in, out_weight, first_gain, up_weight, down_weight, second_gain):
    attended = window_attention(queries, keyvals, head_sink_logit, doc_ids)
    projected = jnp.dot(attended, out_weight, preferred_element_type=jnp.float32)
    first_stream = layer_norm(stream_in.astype(jnp.float32) + projected, first_gain).astype(jnp.bfloat16)
    ff_share = FF // N_TP
    up_groups = up_weight.reshape(D, N_TP, ff_share).transpose(1, 0, 2)
    down_groups = down_weight.reshape(N_TP, ff_share, D)

    def add_group(running, weight_pair):
        up_part, down_part = weight_pair
        hidden = jnp.dot(first_stream, up_part, preferred_element_type=jnp.float32)
        active = jnp.square(jnp.maximum(hidden, 0.0)).astype(jnp.bfloat16)
        partial_value = jnp.dot(active, down_part, preferred_element_type=jnp.float32)
        rounded = lax.optimization_barrier(partial_value.astype(jnp.bfloat16)).astype(jnp.float32)
        return (running + rounded, None)
    mixed_out, unused_out = lax.scan(add_group, jnp.zeros((PACKED_TOKENS, D), jnp.float32), (up_groups, down_groups))
    return layer_norm(first_stream.astype(jnp.float32) + mixed_out, second_gain).astype(jnp.bfloat16)
```

```python
import jax
import jax.numpy as jnp
from jax import lax
from jax.experimental import pallas as pl
from jax.experimental.pallas import tpu as pltpu
from jax.sharding import PartitionSpec as P

MESH = pl.DeviceIdType.MESH
F32 = jnp.float32
BF16 = jnp.bfloat16
NEG_LARGE = -1e30
NORM_EPS = 1e-05
R = 4
BLK = 128
D = 2048
HID = 1024
NCH = 8
CW = D // NCH

ORDER = [
    (0, 0), (1, 0), (3, 0), (0, 1), (0, 3), (3, 3), (3, 1), (1, 1),
    (1, 3), (2, 0), (0, 2), (3, 2), (2, 3), (2, 1), (1, 2), (2, 2),
]
RANK = {o: i for i, o in enumerate(ORDER)}


def nt_dot(a, b):
    return lax.dot_general(a, b, (((1,), (1,)), ((), ())), preferred_element_type=F32)


def dot(a, b):
    return jnp.dot(a, b, preferred_element_type=F32)


def normed(x, gain):
    centre = jnp.mean(x, axis=-1, keepdims=True)
    shifted = x - centre
    spread = jnp.mean(shifted * shifted, axis=-1, keepdims=True)
    return shifted * lax.rsqrt(spread + NORM_EPS) * gain


class Sems:
    def __init__(self):
        self.index = {}

    def at(self, key, count=1):
        if key not in self.index:
            self.index[key] = (sum(c for _, c in self.index.values()), count)
        return self.index[key][0]


def kernel(
    q_h, kv_h, sink_s, doc_h, st_h, ow_h, g1, up_h, dn_h, g2, out,
    qv, kvx, docv, doc_l, doc_r, docx, stv, owv, att_own, att_all, xbuf,
    up_all, dn_all, fs, act, psend, prx, pown, s1, s2, s3, mid_l, mid_r, fin_l, fin_r, macc,
    ss, rs, ls,
):
    sp, tp = lax.axis_index("sp"), lax.axis_index("tp")
    z, y = sp // R, sp % R
    x, core = tp // 2, tp % 2
    stride_a, stride_b = 1 + 3 * core, 4 - 3 * core
    a = y * (1 - core) + z * core
    b = z * (1 - core) + y * core

    def sp_of(da, db):
        return ((a + da) % R) * stride_a + ((b + db) % R) * stride_b

    partner = (sp, x * 2 + (1 - core))
    right = (sp, ((x + 1) % R) * 2 + core)
    left = (sp, ((x + R - 1) % R) * 2 + core)
    sp_next, sp_prev = (sp + 1) % 16, (sp + 15) % 16

    local_names = ["kv", "doc", "q", "up", "dn", "st", "ow"]
    own_up = up_all.at[pl.ds(pl.multiple_of(sp * BLK, BLK), BLK), :]
    pairs = {
        "kv": (kv_h, kvx.at[pl.ds(BLK, 1024), :]),
        "doc": (doc_h, docv),
        "q": (q_h, qv),
        "up": (up_h, own_up),
        "dn": (dn_h, dn_all.at[:, pl.ds(0, BLK)]),
        "st": (st_h, stv),
        "ow": (ow_h, owv),
    }
    local = {n: pltpu.make_async_copy(*pairs[n], ls.at[i]) for i, n in enumerate(local_names)}
    for n in local_names:
        local[n].start()

    barrier = pltpu.get_barrier_semaphore()
    greet = [(sp, (tp + i) % 8) for i in range(1, 8)]
    greet += [(sp_of(da, db), tp) for da, db in ((1, 0), (3, 0), (0, 1), (0, 3))]
    greet += [(sp_next, tp), (sp_prev, tp)]
    for dev in greet:
        pl.semaphore_signal(barrier, inc=1, device_id=dev, device_id_type=MESH)
    pl.semaphore_wait(barrier, len(greet))

    sems = Sems()
    sent = []
    waited = set()
    arriving = {}

    def send(key, src, dst, dev):
        i = sems.at(key)
        copy = pltpu.make_async_remote_copy(
            src_ref=src, dst_ref=dst, send_sem=ss.at[i], recv_sem=rs.at[i], device_id=dev, device_id_type=MESH
        )
        copy.start()
        sent.append(copy)
        arriving[key] = copy

    def arrive(key):
        if key not in waited:
            waited.add(key)
            arriving[key].wait_recv()

    local["kv"].wait()
    local["doc"].wait()
    send("kv_l", kvx.at[pl.ds(1024, BLK), :], kvx.at[pl.ds(0, BLK), :], (sp_next, tp))
    send("kv_r", kvx.at[pl.ds(BLK, BLK), :], kvx.at[pl.ds(1024 + BLK, BLK), :], (sp_prev, tp))
    send("doc_l", docv, doc_l, (sp_next, tp))
    send("doc_r", docv, doc_r, (sp_prev, tp))

    def block(w, origin, at, half):
        da, db = origin
        if w == "u":
            lo, n = {None: (0, BLK), 0: (0, BLK // 2), 1: (BLK // 2, BLK // 2)}[half]
            return up_all.at[pl.ds(pl.multiple_of(sp_of(da, db) * BLK + lo, BLK // 2), n), :]
        lo, n = {None: (0, HID), 0: (0, HID // 2), 1: (HID // 2, HID // 2)}[half]
        ra, rb = (da - at[0]) % R, (db - at[1]) % R
        r0, r1 = RANK[(ra, rb)], RANK[(rb, ra)]
        slot = r0 + core * (r1 - r0)
        return dn_all.at[pl.ds(lo, n), pl.ds(pl.multiple_of(slot * BLK, BLK), BLK)]

    def pass_on(w, origin, to, half=None):
        rel = ((origin[0] - to[0]) % R, (origin[1] - to[1]) % R)
        send(
            (w, rel, half), block(w, origin, (0, 0), half), block(w, origin, to, half),
            (sp_of(to[0] % R, to[1] % R), tp),
        )

    AP, AM, BP, BM = (1, 0), (-1, 0), (0, 1), (0, -1)
    relayed = set()

    def need(w, origin):
        if (w, origin) in relayed:
            return
        relayed.add((w, origin))
        if origin == (2, 0):
            arrive((w, origin, 0))
            arrive((w, origin, 1))
        else:
            arrive((w, origin, None))
        if origin == (3, 0):
            pass_on(w, origin, AP, 0)
        if origin == (1, 0):
            pass_on(w, origin, AM, 1)
        if origin in ((3, 0), (1, 0), (2, 0)):
            pass_on(w, origin, BP)
            pass_on(w, origin, BM)
        if origin in ((0, 3), (2, 3)):
            pass_on(w, origin, BP)
        if origin in ((3, 1), (1, 1)):
            pass_on(w, origin, BM)

    local["up"].wait()
    for to in (AP, AM, BP, BM):
        pass_on("u", (0, 0), to)
    local["dn"].wait()
    for to in (AP, AM):
        pass_on("d", (0, 0), to)

    local["q"].wait()
    docx[pl.ds(8, 8), :] = docv[...].astype(F32)
    row = lax.broadcasted_iota(jnp.int32, (BLK, BLK), 0)
    col = lax.broadcasted_iota(jnp.int32, (BLK, BLK), 1)
    low = col < 64
    a2a = sems.at("a2a", 8)

    def attend(blk):
        rows = pl.ds(pl.multiple_of(blk * BLK, BLK), BLK)
        qf = qv[rows, :].astype(F32) * 0.125
        q2 = jnp.concatenate(
            [jnp.where(low, qf, 0.0), jnp.where(low, pltpu.roll(qf, 64, 1), 0.0)], axis=0
        ).astype(BF16)
        kvb = kvx[pl.ds(pl.multiple_of(blk * BLK, BLK), 3 * BLK), :]
        s = nt_dot(q2, kvb)
        dq = jnp.broadcast_to(docx[pl.ds(blk + 8, 1), :], (BLK, BLK)).T
        same = [jnp.broadcast_to(docx[pl.ds(blk + 7 + j, 1), :], (BLK, BLK)) == dq for j in range(3)]
        same[0] = same[0] & (col >= row)
        same[2] = same[2] & (col <= row)
        weights, scale = [], []
        for h in range(2):
            sink = sink_s[h]
            t = [
                jnp.where(same[j], s[h * BLK : (h + 1) * BLK, j * BLK : (j + 1) * BLK], NEG_LARGE)
                for j in range(3)
            ]
            top = jnp.max(jnp.maximum(jnp.maximum(t[0], t[1]), t[2]), axis=-1, keepdims=True)
            top = jnp.maximum(top, sink)
            p = [jnp.exp(v - top) for v in t]
            total = jnp.sum(p[0] + p[1] + p[2], axis=-1, keepdims=True) + jnp.exp(sink - top)
            weights.append(jnp.concatenate(p, axis=1).astype(BF16))
            scale.append(1.0 / total)
        o = dot(jnp.concatenate(weights, axis=0), kvb)
        o0, o1 = o[:BLK] * scale[0], o[BLK:] * scale[1]
        att_own[rows, :] = jnp.where(low, pltpu.roll(o0, 64, 1), o1).astype(BF16)
        mine = pl.ds(pl.multiple_of(tp * BLK, BLK), BLK)

        @pl.when(blk != tp)
        def _():
            pltpu.make_async_remote_copy(
                src_ref=att_own.at[rows, :], dst_ref=att_all.at[:, mine],
                send_sem=ss.at[a2a + blk], recv_sem=rs.at[a2a + tp],
                device_id=(sp, blk), device_id_type=MESH,
            ).start()

        @pl.when(blk == tp)
        def _():
            att_all[:, mine] = att_own[rows, :]

    def inner(i, carry):
        attend(i)
        return carry

    lax.fori_loop(1, 7, inner, 0)
    for key in ("kv_l", "kv_r", "doc_l", "doc_r"):
        arrive(key)
    docx[pl.ds(0, 8), :] = jnp.where(sp == 0, -1.0, doc_l[...].astype(F32))
    docx[pl.ds(16, 8), :] = jnp.where(sp == 15, -1.0, doc_r[...].astype(F32))

    def outer(i, carry):
        attend(i * 7)
        return carry

    lax.fori_loop(0, 2, outer, 0)

    def a2a_copy(i):
        other = (tp + i) % 8
        return pltpu.make_async_remote_copy(
            src_ref=att_own.at[pl.ds(pl.multiple_of(other * BLK, BLK), BLK), :],
            dst_ref=att_all.at[:, pl.ds(pl.multiple_of(other * BLK, BLK), BLK)],
            send_sem=ss.at[a2a + other], recv_sem=rs.at[a2a + other],
            device_id=(sp, other), device_id_type=MESH,
        )

    local["ow"].wait()
    local["st"].wait()
    for i in range(1, 8):
        a2a_copy(i).wait_recv()

    def project(n, carry):
        cols = pl.ds(pl.multiple_of(n * 256, 256), 256)
        xbuf[:, cols] = dot(att_all[...], owv[:, cols]) + stv[:, cols].astype(F32)
        return carry

    lax.fori_loop(0, 8, project, 0)
    need("u", (3, 0))
    need("u", (1, 0))
    need("u", (0, 3))

    HALF = BLK // 2
    half = lambda h: pl.ds(h * HALF, HALF)

    def fs_send(name, src, dst, h, dev):
        send((name, h), fs.at[src[0], src[1], half(h), :], fs.at[dst[0], dst[1], half(h), :], dev)

    for h in range(2):
        fs[0, 0, half(h), :] = normed(xbuf[half(h), :], g1[...]).astype(BF16)
        if h == 0:
            fs_send("x_l", (0, 0), (0, 3), 0, right)
    fs_send("x_r", (0, 0), (0, 1), 1, left)
    fs_send("x_l", (0, 0), (0, 3), 1, right)
    fs_send("x_r", (0, 0), (0, 1), 0, left)
    for h in range(2):
        fs_send("c0", (0, 0), (1, 0), h, partner)

    def gather_rows(name, h):
        arrive((name, h))
        if name == "x_l":
            if h == 0:
                fs_send("x_2", (0, 3), (0, 2), 0, right)
            fs_send("c3", (0, 3), (1, 3), h, partner)
        elif name == "x_r":
            if h == 1:
                fs_send("x_2", (0, 1), (0, 2), 1, left)
            fs_send("c1", (0, 1), (1, 1), h, partner)
        elif name == "x_2":
            fs_send("c2", (0, 2), (1, 2), h, partner)

    def hidden(dx):
        for h in range(2):
            arrive((f"c{dx}", h))

        def part(n, carry):
            cols = pl.ds(pl.multiple_of(n * 256, 256), 256)
            rows = fs[:, dx].reshape(2 * BLK, D)
            v = jnp.maximum(dot(rows, up_all[:, cols]), 0.0)
            act[:, dx, :, cols] = (v * v).astype(BF16).reshape(2, BLK, 256)
            return carry

        lax.fori_loop(0, HID // 256, part, 0)

    need("u", (2, 0))
    for to in (BP, BM):
        pass_on("d", (0, 0), to)
    need("d", (3, 0))
    need("d", (1, 0))
    need("u", (3, 1))
    gather_rows("x_l", 0)
    gather_rows("x_r", 1)
    need("u", (1, 1))
    need("d", (0, 3))
    need("u", (2, 3))
    need("d", (2, 0))
    gather_rows("x_l", 1)
    gather_rows("x_r", 0)
    for da in range(R):
        for db in range(R):
            if (da, db) != (0, 0):
                need("u", (da, db))
    hidden(0)
    hidden(1)
    need("d", (3, 1))
    hidden(3)
    gather_rows("x_2", 0)
    gather_rows("x_2", 1)
    hidden(2)

    def cols_of(rank):
        dy, dz = ORDER[rank]
        return pl.ds(pl.multiple_of((((z + dz) % R) * R + (y + dy) % R) * BLK, BLK), BLK)

    def product(j):
        for o in (ORDER[2 * j], ORDER[2 * j + 1]):
            for origin in (o, (o[1], o[0])):
                if origin != (0, 0):
                    need("d", origin)
        cols = pl.ds(j * CW, CW)
        psend[j] = dot(act[1].reshape(4 * BLK, HID), dn_all[:, cols]).astype(BF16).reshape(R, BLK, CW)
        send(("p", j), psend.at[j], prx.at[j], partner)
        pown[j] = dot(act[0].reshape(4 * BLK, HID), dn_all[:, cols]).reshape(R, BLK, CW)

    def pair_sum(j):
        arrive(("p", j))
        s2[j] = (pown[j, 2] + prx[j, 2].astype(F32)).astype(BF16)
        send(("mid_l", j), s2.at[j, pl.ds(0, HALF), :], mid_l.at[j], right)
        send(("mid_r", j), s2.at[j, pl.ds(HALF, HALF), :], mid_r.at[j], left)
        mine = pown[j, 0] + prx[j, 0].astype(F32)
        for i in range(2):
            macc[:, cols_of(2 * j + i)] = mine[:, i * BLK : (i + 1) * BLK]

    def middle(j):
        lo, hi = pl.ds(0, HALF), pl.ds(HALF, HALF)
        s1[j, hi, :] = (pown[j, 1, hi, :] + prx[j, 1, hi, :].astype(F32)).astype(BF16)
        s3[j, lo, :] = (pown[j, 3, lo, :] + prx[j, 3, lo, :].astype(F32)).astype(BF16)
        arrive(("mid_l", j))
        s1[j, lo, :] = (pown[j, 1, lo, :] + prx[j, 1, lo, :].astype(F32) + mid_l[j].astype(F32)).astype(BF16)
        send(("fin_l", j), s1.at[j], fin_l.at[j], right)
        arrive(("mid_r", j))
        s3[j, hi, :] = (pown[j, 3, hi, :] + prx[j, 3, hi, :].astype(F32) + mid_r[j].astype(F32)).astype(BF16)
        send(("fin_r", j), s3.at[j], fin_r.at[j], left)

    def total_sum(j):
        arrive(("fin_l", j))
        arrive(("fin_r", j))
        v = fin_l[j].astype(F32) + fin_r[j].astype(F32)
        for i in range(2):
            macc[:, cols_of(2 * j + i)] += v[:, i * BLK : (i + 1) * BLK]

    for i in range(NCH + 6):
        if i < NCH:
            product(i)
        if 0 <= i - 1 < NCH:
            pair_sum(i - 1)
        if 0 <= i - 3 < NCH:
            middle(i - 3)
        if 0 <= i - 6 < NCH:
            total_sum(i - 6)

    for h in range(2):
        v = fs[0, 0, half(h), :].astype(F32) + macc[half(h), :]
        out[half(h), :] = normed(v, g2[...]).astype(BF16)

    for copy in sent:
        copy.wait_send()
    for i in range(1, 8):
        a2a_copy(i).wait_send()


def per_device(q, kv, sink, doc, stream, ow, g1, up, dn, g2):
    vm, anyw = pl.BlockSpec(memory_space=pltpu.VMEM), pl.BlockSpec(memory_space=pl.ANY)
    smem = pl.BlockSpec(memory_space=pltpu.SMEM)
    return pl.pallas_call(
        kernel,
        out_shape=jax.ShapeDtypeStruct(stream.shape, BF16),
        in_specs=[anyw, anyw, smem, anyw, anyw, anyw, vm, anyw, anyw, vm],
        out_specs=vm,
        scratch_shapes=[
            pltpu.VMEM((1024, BLK), BF16),
            pltpu.VMEM((1024 + 2 * BLK, BLK), BF16),
            pltpu.VMEM((8, BLK), jnp.int32),
            pltpu.VMEM((8, BLK), jnp.int32),
            pltpu.VMEM((8, BLK), jnp.int32),
            pltpu.VMEM((24, BLK), F32),
            pltpu.VMEM((BLK, D), BF16),
            pltpu.VMEM((1024, D), BF16),
            pltpu.VMEM((1024, BLK), BF16),
            pltpu.VMEM((BLK, 1024), BF16),
            pltpu.VMEM((BLK, D), F32),
            pltpu.VMEM((D, HID), BF16),
            pltpu.VMEM((HID, D), BF16),
            pltpu.VMEM((2, R, BLK, D), BF16),
            pltpu.VMEM((2, R, BLK, HID), BF16),
            pltpu.VMEM((NCH, R, BLK, CW), BF16),
            pltpu.VMEM((NCH, R, BLK, CW), BF16),
            pltpu.VMEM((NCH, R, BLK, CW), F32),
            pltpu.VMEM((NCH, BLK, CW), BF16),
            pltpu.VMEM((NCH, BLK, CW), BF16),
            pltpu.VMEM((NCH, BLK, CW), BF16),
            pltpu.VMEM((NCH, BLK // 2, CW), BF16),
            pltpu.VMEM((NCH, BLK // 2, CW), BF16),
            pltpu.VMEM((NCH, BLK, CW), BF16),
            pltpu.VMEM((NCH, BLK, CW), BF16),
            pltpu.VMEM((BLK, D), F32),
            pltpu.SemaphoreType.DMA((112,)),
            pltpu.SemaphoreType.DMA((112,)),
            pltpu.SemaphoreType.DMA((8,)),
        ],
        compiler_params=pltpu.CompilerParams(
            collective_id=0, has_side_effects=True, vmem_limit_bytes=60 * 1024 * 1024
        ),
        name="layer",
    )(
        q, kv.reshape(1024, BLK), sink, doc.reshape(8, BLK), stream, ow, g1.reshape(1, D), up, dn, g2.reshape(1, D)
    )


def solution(mesh):
    placed = (
        P("sp", "tp"),
        P("sp", "tp", None),
        P("tp"),
        P("sp"),
        P(("sp", "tp"), None),
        P(),
        P(),
        P("sp", "tp"),
        P("tp", "sp"),
        P(),
    )
    return jax.shard_map(
        per_device, mesh=mesh, in_specs=placed, out_specs=P(("sp", "tp"), None), check_vma=False
    )
```

```python
import functools

import jax
import jax.numpy as jnp
from jax import lax
from jax.experimental import pallas as pl
from jax.experimental.pallas import tpu as pltpu
from jax.sharding import PartitionSpec as P

MESH = pl.DeviceIdType.MESH
F32 = jnp.float32
BF16 = jnp.bfloat16
NEG_LARGE = -1e30
NORM_EPS = 1e-05
R = 4
BLK = 128
D = 2048
HID = 1024
NCH = 8
CW = D // NCH

ORDER = [
    (0, 0), (1, 0), (3, 0), (0, 1), (0, 3), (3, 3), (3, 1), (1, 1),
    (1, 3), (2, 0), (0, 2), (3, 2), (2, 3), (2, 1), (1, 2), (2, 2),
]
RANK = {o: i for i, o in enumerate(ORDER)}


def nt_dot(a, b):
    return lax.dot_general(a, b, (((1,), (1,)), ((), ())), preferred_element_type=F32)


def dot(a, b):
    return jnp.dot(a, b, preferred_element_type=F32)


def normed(x, gain):
    centre = jnp.mean(x, axis=-1, keepdims=True)
    shifted = x - centre
    spread = jnp.mean(shifted * shifted, axis=-1, keepdims=True)
    return shifted * lax.rsqrt(spread + NORM_EPS) * gain


def scoped(name):
    def wrap(f):
        @functools.wraps(f)
        def run(*args):
            tag = "_".join("".join(c for c in str(v) if c.isalnum()) for v in args if isinstance(v, (int, str, tuple)))
            with jax.named_scope(f"{name}#v={tag}"):
                return f(*args)

        return run

    return wrap


class Sems:
    def __init__(self):
        self.index = {}

    def at(self, key, count=1):
        if key not in self.index:
            self.index[key] = (sum(c for _, c in self.index.values()), count)
        return self.index[key][0]


def kernel(
    q_h, kv_h, sink_s, doc_h, st_h, ow_h, g1, up_h, dn_h, g2, out,
    qv, kvx, docv, doc_l, doc_r, docx, stv, owv, att_own, att_all, xbuf,
    up_all, dn_all, fs, act, psend, prx, pown, s1, s2, s3, mid_l, mid_r, fin_l, fin_r, macc,
    ss, rs, ls,
):
    sp, tp = lax.axis_index("sp"), lax.axis_index("tp")
    z, y = sp // R, sp % R
    x, core = tp // 2, tp % 2
    stride_a, stride_b = 1 + 3 * core, 4 - 3 * core
    a = y * (1 - core) + z * core
    b = z * (1 - core) + y * core

    def sp_of(da, db):
        return ((a + da) % R) * stride_a + ((b + db) % R) * stride_b

    partner = (sp, x * 2 + (1 - core))
    right = (sp, ((x + 1) % R) * 2 + core)
    left = (sp, ((x + R - 1) % R) * 2 + core)
    sp_next, sp_prev = (sp + 1) % 16, (sp + 15) % 16

    local_names = ["kv", "doc", "q", "up", "dn", "st", "ow"]
    own_up = up_all.at[pl.ds(pl.multiple_of(sp * BLK, BLK), BLK), :]
    pairs = {
        "kv": (kv_h, kvx.at[pl.ds(BLK, 1024), :]),
        "doc": (doc_h, docv),
        "q": (q_h, qv),
        "up": (up_h, own_up),
        "dn": (dn_h, dn_all.at[:, pl.ds(0, BLK)]),
        "st": (st_h, stv),
        "ow": (ow_h, owv),
    }
    local = {n: pltpu.make_async_copy(*pairs[n], ls.at[i]) for i, n in enumerate(local_names)}
    for n in local_names:
        local[n].start()

    barrier = pltpu.get_barrier_semaphore()
    greet = [(sp, (tp + i) % 8) for i in range(1, 8)]
    greet += [(sp_of(da, db), tp) for da, db in ((1, 0), (3, 0), (0, 1), (0, 3))]
    greet += [(sp_next, tp), (sp_prev, tp)]
    for dev in greet:
        pl.semaphore_signal(barrier, inc=1, device_id=dev, device_id_type=MESH)
    pl.semaphore_wait(barrier, len(greet))

    sems = Sems()
    sent = []
    waited = set()
    arriving = {}

    def send(key, src, dst, dev):
        i = sems.at(key)
        copy = pltpu.make_async_remote_copy(
            src_ref=src, dst_ref=dst, send_sem=ss.at[i], recv_sem=rs.at[i], device_id=dev, device_id_type=MESH
        )
        copy.start()
        sent.append(copy)
        arriving[key] = copy

    def arrive(key):
        if key not in waited:
            waited.add(key)
            arriving[key].wait_recv()

    local["kv"].wait()
    local["doc"].wait()
    send("kv_l", kvx.at[pl.ds(1024, BLK), :], kvx.at[pl.ds(0, BLK), :], (sp_next, tp))
    send("kv_r", kvx.at[pl.ds(BLK, BLK), :], kvx.at[pl.ds(1024 + BLK, BLK), :], (sp_prev, tp))
    send("doc_l", docv, doc_l, (sp_next, tp))
    send("doc_r", docv, doc_r, (sp_prev, tp))

    def block(w, origin, at, half):
        da, db = origin
        if w == "u":
            lo, n = {None: (0, BLK), 0: (0, BLK // 2), 1: (BLK // 2, BLK // 2)}[half]
            return up_all.at[pl.ds(pl.multiple_of(sp_of(da, db) * BLK + lo, BLK // 2), n), :]
        lo, n = {None: (0, HID), 0: (0, HID // 2), 1: (HID // 2, HID // 2)}[half]
        ra, rb = (da - at[0]) % R, (db - at[1]) % R
        r0, r1 = RANK[(ra, rb)], RANK[(rb, ra)]
        slot = r0 + core * (r1 - r0)
        return dn_all.at[pl.ds(lo, n), pl.ds(pl.multiple_of(slot * BLK, BLK), BLK)]

    def pass_on(w, origin, to, half=None):
        rel = ((origin[0] - to[0]) % R, (origin[1] - to[1]) % R)
        send(
            (w, rel, half), block(w, origin, (0, 0), half), block(w, origin, to, half),
            (sp_of(to[0] % R, to[1] % R), tp),
        )

    AP, AM, BP, BM = (1, 0), (-1, 0), (0, 1), (0, -1)
    relayed = set()

    @scoped("need")
    def need(w, origin):
        if (w, origin) in relayed:
            return
        relayed.add((w, origin))
        if origin == (2, 0):
            arrive((w, origin, 0))
            arrive((w, origin, 1))
        else:
            arrive((w, origin, None))
        if origin == (3, 0):
            pass_on(w, origin, AP, 0)
        if origin == (1, 0):
            pass_on(w, origin, AM, 1)
        if origin in ((3, 0), (1, 0), (2, 0)):
            pass_on(w, origin, BP)
            pass_on(w, origin, BM)
        if origin in ((0, 3), (2, 3)):
            pass_on(w, origin, BP)
        if origin in ((3, 1), (1, 1)):
            pass_on(w, origin, BM)
        if (w, origin) == ("u", (1, 1)):
            local["dn"].wait()
            pass_on("d", (0, 0), BP)
            pass_on("d", (0, 0), BM)
        if (w, origin) == ("u", (2, 3)):
            pass_on("d", (0, 0), AP)
            pass_on("d", (0, 0), AM)

    local["up"].wait()
    for to in (AP, AM):
        pass_on("u", (0, 0), to)

    local["q"].wait()
    docx[pl.ds(8, 8), :] = docv[...].astype(F32)
    row = lax.broadcasted_iota(jnp.int32, (BLK, BLK), 0)
    col = lax.broadcasted_iota(jnp.int32, (BLK, BLK), 1)
    low = col < 64
    a2a = sems.at("a2a", 8)

    def attended(blk):
        rows = pl.ds(pl.multiple_of(blk * BLK, BLK), BLK)
        qf = qv[rows, :].astype(F32) * 0.125
        q2 = jnp.concatenate(
            [jnp.where(low, qf, 0.0), jnp.where(low, pltpu.roll(qf, 64, 1), 0.0)], axis=0
        ).astype(BF16)
        kvb = kvx[pl.ds(pl.multiple_of(blk * BLK, BLK), 3 * BLK), :]
        s = nt_dot(q2, kvb)
        dq = jnp.broadcast_to(docx[pl.ds(blk + 8, 1), :], (BLK, BLK)).T
        same = [jnp.broadcast_to(docx[pl.ds(blk + 7 + j, 1), :], (BLK, BLK)) == dq for j in range(3)]
        same[0] = same[0] & (col >= row)
        same[2] = same[2] & (col <= row)
        weights, scale = [], []
        for h in range(2):
            sink = sink_s[h]
            t = [
                jnp.where(same[j], s[h * BLK : (h + 1) * BLK, j * BLK : (j + 1) * BLK], NEG_LARGE)
                for j in range(3)
            ]
            top = jnp.max(jnp.maximum(jnp.maximum(t[0], t[1]), t[2]), axis=-1, keepdims=True)
            top = jnp.maximum(top, sink)
            p = [jnp.exp(v - top) for v in t]
            total = jnp.sum(p[0] + p[1] + p[2], axis=-1, keepdims=True) + jnp.exp(sink - top)
            weights.append(jnp.concatenate(p, axis=1).astype(BF16))
            scale.append(1.0 / total)
        o = dot(jnp.concatenate(weights, axis=0), kvb)
        o0, o1 = o[:BLK] * scale[0], o[BLK:] * scale[1]
        return jnp.where(low, pltpu.roll(o0, 64, 1), o1).astype(BF16)

    def hand_out(blk):
        rows = pl.ds(pl.multiple_of(blk * BLK, BLK), BLK)
        mine = pl.ds(pl.multiple_of(tp * BLK, BLK), BLK)

        @pl.when(blk != tp)
        def _():
            pltpu.make_async_remote_copy(
                src_ref=att_own.at[rows, :], dst_ref=att_all.at[:, mine],
                send_sem=ss.at[a2a + blk], recv_sem=rs.at[a2a + tp],
                device_id=(sp, blk), device_id_type=MESH,
            ).start()

        @pl.when(blk == tp)
        def _():
            att_all[:, mine] = att_own[rows, :]

    @scoped("attend")
    def attend(first, second):
        values = [attended(first), attended(second)]
        for blk, v in zip((first, second), values):
            att_own[pl.ds(pl.multiple_of(blk * BLK, BLK), BLK), :] = v
        for blk in (first, second):
            hand_out(blk)

    def inner(i, carry):
        attend(2 * i + 1, 2 * i + 2)
        return carry

    lax.fori_loop(0, 2, inner, 0)
    for to in (BP, BM):
        pass_on("u", (0, 0), to)
    lax.fori_loop(2, 3, inner, 0)
    for key in ("kv_l", "kv_r", "doc_l", "doc_r"):
        arrive(key)
    docx[pl.ds(0, 8), :] = jnp.where(sp == 0, -1.0, doc_l[...].astype(F32))
    docx[pl.ds(16, 8), :] = jnp.where(sp == 15, -1.0, doc_r[...].astype(F32))

    def outer(i, carry):
        attend(i, i + 7)
        return carry

    lax.fori_loop(0, 1, outer, 0)
    need("u", (3, 0))
    need("u", (1, 0))

    def a2a_copy(i):
        other = (tp + i) % 8
        return pltpu.make_async_remote_copy(
            src_ref=att_own.at[pl.ds(pl.multiple_of(other * BLK, BLK), BLK), :],
            dst_ref=att_all.at[:, pl.ds(pl.multiple_of(other * BLK, BLK), BLK)],
            send_sem=ss.at[a2a + other], recv_sem=rs.at[a2a + other],
            device_id=(sp, other), device_id_type=MESH,
        )

    @scoped("a2a_wait")
    def a2a_wait():
        local["ow"].wait()
        local["st"].wait()
        for i in range(1, 8):
            a2a_copy(i).wait_recv()

    a2a_wait()

    def project(n):
        cols = pl.ds(n * 512, 512)
        xbuf[:, cols] = dot(att_all[...], owv[:, cols]) + stv[:, cols].astype(F32)

    @scoped("projection")
    def projection():
        for n in range(4):
            project(n)

    projection()
    need("u", (0, 3))

    HALF = BLK // 2
    half = lambda h: pl.ds(h * HALF, HALF)

    def fs_send(name, src, dst, h, dev):
        send((name, h), fs.at[src[0], src[1], half(h), :], fs.at[dst[0], dst[1], half(h), :], dev)

    @scoped("first_norm")
    def first_norm(h):
        fs[0, 0, half(h), :] = normed(xbuf[half(h), :], g1[...]).astype(BF16)

    for h in range(2):
        first_norm(h)
        if h == 0:
            fs_send("x_l", (0, 0), (0, 3), 0, right)
    fs_send("x_r", (0, 0), (0, 1), 1, left)
    fs_send("x_l", (0, 0), (0, 3), 1, right)
    fs_send("x_r", (0, 0), (0, 1), 0, left)
    for h in range(2):
        fs_send("c0", (0, 0), (1, 0), h, partner)

    @scoped("gather_rows")
    def gather_rows(name, h):
        arrive((name, h))
        if name == "x_l":
            if h == 0:
                fs_send("x_2", (0, 3), (0, 2), 0, right)
            fs_send("c3", (0, 3), (1, 3), h, partner)
        elif name == "x_r":
            if h == 1:
                fs_send("x_2", (0, 1), (0, 2), 1, left)
            fs_send("c1", (0, 1), (1, 1), h, partner)
        elif name == "x_2":
            fs_send("c2", (0, 2), (1, 2), h, partner)

    @scoped("hidden")
    def hidden(dx):
        for h in range(2):
            arrive((f"c{dx}", h))

        for n in range(HID // 256):
            cols = pl.ds(n * 256, 256)
            rows = fs[:, dx].reshape(2 * BLK, D)
            v = jnp.maximum(dot(rows, up_all[:, cols]), 0.0)
            act[:, dx, :, cols] = (v * v).astype(BF16).reshape(2, BLK, 256)

    need("u", (2, 0))
    need("u", (3, 1))
    need("u", (1, 1))
    gather_rows("x_l", 0)
    gather_rows("x_r", 1)
    need("u", (2, 3))
    gather_rows("x_l", 1)
    gather_rows("x_r", 0)
    need("d", (0, 3))
    need("d", (3, 0))
    need("d", (1, 0))
    gather_rows("x_2", 0)
    gather_rows("x_2", 1)
    for da in range(R):
        for db in range(R):
            if (da, db) != (0, 0):
                need("u", (da, db))
    hidden(0)
    hidden(1)
    need("d", (2, 0))
    hidden(3)
    need("d", (3, 1))
    hidden(2)

    def cols_of(rank):
        dy, dz = ORDER[rank]
        return pl.ds(pl.multiple_of((((z + dz) % R) * R + (y + dy) % R) * BLK, BLK), BLK)

    @scoped("product")
    def product(j):
        for o in (ORDER[2 * j], ORDER[2 * j + 1]):
            for origin in (o, (o[1], o[0])):
                if origin != (0, 0):
                    need("d", origin)
        cols = pl.ds(j * CW, CW)
        psend[j] = dot(act[1].reshape(4 * BLK, HID), dn_all[:, cols]).astype(BF16).reshape(R, BLK, CW)
        send(("p", j), psend.at[j], prx.at[j], partner)
        pown[j] = dot(act[0].reshape(4 * BLK, HID), dn_all[:, cols]).reshape(R, BLK, CW)

    @scoped("pair_sum")
    def pair_sum(j):
        arrive(("p", j))
        s2[j] = (pown[j, 2] + prx[j, 2].astype(F32)).astype(BF16)
        send(("mid_l", j), s2.at[j, pl.ds(0, HALF), :], mid_l.at[j], right)
        send(("mid_r", j), s2.at[j, pl.ds(HALF, HALF), :], mid_r.at[j], left)
        mine = pown[j, 0] + prx[j, 0].astype(F32)
        for i in range(2):
            macc[:, cols_of(2 * j + i)] = mine[:, i * BLK : (i + 1) * BLK]

    @scoped("middle")
    def middle(j):
        lo, hi = pl.ds(0, HALF), pl.ds(HALF, HALF)
        s1[j, hi, :] = (pown[j, 1, hi, :] + prx[j, 1, hi, :].astype(F32)).astype(BF16)
        s3[j, lo, :] = (pown[j, 3, lo, :] + prx[j, 3, lo, :].astype(F32)).astype(BF16)
        arrive(("mid_l", j))
        s1[j, lo, :] = (pown[j, 1, lo, :] + prx[j, 1, lo, :].astype(F32) + mid_l[j].astype(F32)).astype(BF16)
        send(("fin_l", j), s1.at[j], fin_l.at[j], right)
        arrive(("mid_r", j))
        s3[j, hi, :] = (pown[j, 3, hi, :] + prx[j, 3, hi, :].astype(F32) + mid_r[j].astype(F32)).astype(BF16)
        send(("fin_r", j), s3.at[j], fin_r.at[j], left)

    @scoped("total_sum")
    def total_sum(j):
        arrive(("fin_l", j))
        arrive(("fin_r", j))
        v = fin_l[j].astype(F32) + fin_r[j].astype(F32)
        for i in range(2):
            macc[:, cols_of(2 * j + i)] += v[:, i * BLK : (i + 1) * BLK]

    for i in range(NCH + 6):
        if i < NCH:
            product(i)
        if 0 <= i - 1 < NCH:
            pair_sum(i - 1)
        if 0 <= i - 3 < NCH:
            middle(i - 3)
        if 0 <= i - 6 < NCH:
            total_sum(i - 6)

    @scoped("last_norm")
    def last_norm(h):
        v = fs[0, 0, half(h), :].astype(F32) + macc[half(h), :]
        out[half(h), :] = normed(v, g2[...]).astype(BF16)

    for h in range(2):
        last_norm(h)

    @scoped("drain")
    def drain():
        for copy in sent:
            copy.wait_send()
        for i in range(1, 8):
            a2a_copy(i).wait_send()

    drain()


def per_device(q, kv, sink, doc, stream, ow, g1, up, dn, g2):
    vm, anyw = pl.BlockSpec(memory_space=pltpu.VMEM), pl.BlockSpec(memory_space=pl.ANY)
    smem = pl.BlockSpec(memory_space=pltpu.SMEM)
    return pl.pallas_call(
        kernel,
        out_shape=jax.ShapeDtypeStruct(stream.shape, BF16),
        in_specs=[anyw, anyw, smem, anyw, anyw, anyw, vm, anyw, anyw, vm],
        out_specs=vm,
        scratch_shapes=[
            pltpu.VMEM((1024, BLK), BF16),
            pltpu.VMEM((1024 + 2 * BLK, BLK), BF16),
            pltpu.VMEM((8, BLK), jnp.int32),
            pltpu.VMEM((8, BLK), jnp.int32),
            pltpu.VMEM((8, BLK), jnp.int32),
            pltpu.VMEM((24, BLK), F32),
            pltpu.VMEM((BLK, D), BF16),
            pltpu.VMEM((1024, D), BF16),
            pltpu.VMEM((1024, BLK), BF16),
            pltpu.VMEM((BLK, 1024), BF16),
            pltpu.VMEM((BLK, D), F32),
            pltpu.VMEM((D, HID), BF16),
            pltpu.VMEM((HID, D), BF16),
            pltpu.VMEM((2, R, BLK, D), BF16),
            pltpu.VMEM((2, R, BLK, HID), BF16),
            pltpu.VMEM((NCH, R, BLK, CW), BF16),
            pltpu.VMEM((NCH, R, BLK, CW), BF16),
            pltpu.VMEM((NCH, R, BLK, CW), F32),
            pltpu.VMEM((NCH, BLK, CW), BF16),
            pltpu.VMEM((NCH, BLK, CW), BF16),
            pltpu.VMEM((NCH, BLK, CW), BF16),
            pltpu.VMEM((NCH, BLK // 2, CW), BF16),
            pltpu.VMEM((NCH, BLK // 2, CW), BF16),
            pltpu.VMEM((NCH, BLK, CW), BF16),
            pltpu.VMEM((NCH, BLK, CW), BF16),
            pltpu.VMEM((BLK, D), F32),
            pltpu.SemaphoreType.DMA((112,)),
            pltpu.SemaphoreType.DMA((112,)),
            pltpu.SemaphoreType.DMA((8,)),
        ],
        compiler_params=pltpu.CompilerParams(
            collective_id=0, has_side_effects=True, vmem_limit_bytes=60 * 1024 * 1024
        ),
        name="layer",
    )(
        q, kv.reshape(1024, BLK), sink, doc.reshape(8, BLK), stream, ow, g1.reshape(1, D), up, dn, g2.reshape(1, D)
    )


def solution(mesh):
    placed = (
        P("sp", "tp"),
        P("sp", "tp", None),
        P("tp"),
        P("sp"),
        P(("sp", "tp"), None),
        P(),
        P(),
        P("sp", "tp"),
        P("tp", "sp"),
        P(),
    )
    return jax.shard_map(
        per_device, mesh=mesh, in_specs=placed, out_specs=P(("sp", "tp"), None), check_vma=False
    )
```

```python
import functools

import jax
import jax.numpy as jnp
from jax import lax
from jax.experimental import pallas as pl
from jax.experimental.pallas import tpu as pltpu
from jax.sharding import PartitionSpec as P

MESH = pl.DeviceIdType.MESH
F32 = jnp.float32
BF16 = jnp.bfloat16
NEG_LARGE = -1e30
NORM_EPS = 1e-05
R = 4
BLK = 128
D = 2048
HID = 1024
NCH = 8
CW = D // NCH

ORDER = [
    (0, 0), (1, 0), (3, 0), (0, 1), (0, 3), (3, 3), (3, 1), (1, 1),
    (1, 3), (2, 0), (0, 2), (3, 2), (2, 3), (2, 1), (1, 2), (2, 2),
]
RANK = {o: i for i, o in enumerate(ORDER)}

AP, AM, BP, BM = (1, 0), (-1, 0), (0, 1), (0, -1)
ONWARD = {
    (3, 0): [(AP, 0), (BP, None), (BM, None)],
    (1, 0): [(AM, 1), (BP, None), (BM, None)],
    (2, 0): [(BP, None), (BM, None)],
    (0, 3): [(BP, None)],
    (3, 1): [(BM, None)],
    (1, 3): [(BP, 0)],
    (1, 1): [(BM, 1)],
    (2, 3): [(BP, 0)],
    (2, 1): [(BM, 1)],
}
HALVED = ((2, 0), (1, 2), (2, 2))
KA = HID


def nt_dot(a, b):
    return lax.dot_general(a, b, (((1,), (1,)), ((), ())), preferred_element_type=F32)


def dot(a, b):
    return jnp.dot(a, b, preferred_element_type=F32)


def moments(x):
    centre = jnp.mean(x, axis=-1, keepdims=True)
    shifted = x - centre
    return centre, lax.rsqrt(jnp.mean(shifted * shifted, axis=-1, keepdims=True) + NORM_EPS)


def scoped(name):
    def wrap(f):
        @functools.wraps(f)
        def run(*args):
            tag = "_".join("".join(c for c in str(v) if c.isalnum()) for v in args if isinstance(v, (int, str, tuple)))
            with jax.named_scope(f"{name}#v={tag}"):
                return f(*args)

        return run

    return wrap


class Sems:
    def __init__(self):
        self.index = {}

    def at(self, key, count=1):
        if key not in self.index:
            self.index[key] = (sum(c for _, c in self.index.values()), count)
        return self.index[key][0]


def kernel(
    q_h, kv_h, sink_s, doc_h, st_h, ow_h, g1_h, up_h, dn_h, g2_h, out,
    g1, g2, qv, kvx, docv, doc_l, doc_r, docx, stv, owv, att_own, att_all, xbuf,
    up_all, dn_all, fs, hacc, act, psend, prx, pown, s1, s2, s3, mid_l, mid_r, fin_l, fin_r, macc,
    ss, rs, ls,
):
    sp, tp = lax.axis_index("sp"), lax.axis_index("tp")
    z, y = sp // R, sp % R
    x, core = tp // 2, tp % 2
    stride_a, stride_b = 1 + 3 * core, 4 - 3 * core
    a = y * (1 - core) + z * core
    b = z * (1 - core) + y * core

    def sp_of(da, db):
        return ((a + da) % R) * stride_a + ((b + db) % R) * stride_b

    partner = (sp, x * 2 + (1 - core))
    right = (sp, ((x + 1) % R) * 2 + core)
    left = (sp, ((x + R - 1) % R) * 2 + core)
    sp_next, sp_prev = (sp + 1) % 16, (sp + 15) % 16

    local_names = ["kv", "doc", "up", "q", "st", "ow", "dn", "g1", "g2"]
    pairs = {
        "kv": (kv_h, kvx.at[pl.ds(BLK, 1024), :]),
        "doc": (doc_h, docv),
        "q": (q_h, qv),
        "up": (up_h, up_all.at[pl.ds(0, BLK), :]),
        "dn": (dn_h, dn_all.at[:, pl.ds(0, BLK)]),
        "st": (st_h, stv),
        "ow": (ow_h, owv),
        "g1": (g1_h, g1),
        "g2": (g2_h, g2),
    }
    local = {n: pltpu.make_async_copy(*pairs[n], ls.at[i]) for i, n in enumerate(local_names)}
    for n in local_names:
        local[n].start()

    barrier = pltpu.get_barrier_semaphore()
    greet = [(sp, (tp + i) % 8) for i in range(1, 8)]
    greet += [(sp_of(da, db), tp) for da, db in ((1, 0), (3, 0), (0, 1), (0, 3))]
    greet += [(sp_next, tp), (sp_prev, tp)]
    for dev in greet:
        pl.semaphore_signal(barrier, inc=1, device_id=dev, device_id_type=MESH)
    pl.semaphore_wait(barrier, len(greet))

    sems = Sems()
    sent = []
    waited = set()
    arriving = {}

    def send(key, src, dst, dev):
        i = sems.at(key)
        copy = pltpu.make_async_remote_copy(
            src_ref=src, dst_ref=dst, send_sem=ss.at[i], recv_sem=rs.at[i], device_id=dev, device_id_type=MESH
        )
        copy.start()
        sent.append(copy)
        arriving[key] = copy

    def arrive(key):
        if key not in waited:
            waited.add(key)
            arriving[key].wait_recv()

    local["kv"].wait()
    local["doc"].wait()
    send("kv_l", kvx.at[pl.ds(1024, BLK), :], kvx.at[pl.ds(0, BLK), :], (sp_next, tp))
    send("kv_r", kvx.at[pl.ds(BLK, BLK), :], kvx.at[pl.ds(1024 + BLK, BLK), :], (sp_prev, tp))
    send("doc_l", docv, doc_l, (sp_next, tp))
    send("doc_r", docv, doc_r, (sp_prev, tp))

    def block(w, origin, at, half):
        ra, rb = (origin[0] - at[0]) % R, (origin[1] - at[1]) % R
        r0, r1 = RANK[(ra, rb)], RANK[(rb, ra)]
        slot = (r0 + core * (r1 - r0)) * BLK
        size = BLK if w == "u" else HID
        lo, n = {None: (0, size), 0: (0, size // 2), 1: (size // 2, size // 2)}[half]
        if w == "u":
            return up_all.at[pl.ds(pl.multiple_of(slot + lo, BLK // 2), n), :]
        return dn_all.at[pl.ds(lo, n), pl.ds(pl.multiple_of(slot, BLK), BLK)]

    def pass_on(w, origin, to, half=None):
        rel = ((origin[0] - to[0]) % R, (origin[1] - to[1]) % R)
        send(
            (w, rel, half), block(w, origin, (0, 0), half), block(w, origin, to, half),
            (sp_of(to[0] % R, to[1] % R), tp),
        )

    relayed = set()

    @scoped("need")
    def need(w, origin):
        if (w, origin) in relayed:
            return
        relayed.add((w, origin))
        for h in (0, 1) if origin in HALVED else (None,):
            arrive((w, origin, h))
        for to, h in ONWARD.get(origin, ()):
            pass_on(w, origin, to, h)

    def own_down(*ways):
        for to in ways:
            pass_on("d", (0, 0), to)

    local["up"].wait()
    for to in (AP, AM):
        pass_on("u", (0, 0), to)

    local["q"].wait()
    local["dn"].wait()
    docx[pl.ds(8, 8), :] = docv[...].astype(F32)
    row = lax.broadcasted_iota(jnp.int32, (BLK, BLK), 0)
    col = lax.broadcasted_iota(jnp.int32, (BLK, BLK), 1)
    low = col < 64
    a2a = sems.at("a2a", 8)

    def attended(blk):
        rows = pl.ds(pl.multiple_of(blk * BLK, BLK), BLK)
        qf = qv[rows, :].astype(F32) * 0.125
        q2 = jnp.concatenate(
            [jnp.where(low, qf, 0.0), jnp.where(low, pltpu.roll(qf, 64, 1), 0.0)], axis=0
        ).astype(BF16)
        kvb = kvx[pl.ds(pl.multiple_of(blk * BLK, BLK), 3 * BLK), :]
        s = nt_dot(q2, kvb)
        dq = jnp.broadcast_to(docx[pl.ds(blk + 8, 1), :], (BLK, BLK)).T
        same = [jnp.broadcast_to(docx[pl.ds(blk + 7 + j, 1), :], (BLK, BLK)) == dq for j in range(3)]
        same[0] = same[0] & (col >= row)
        same[2] = same[2] & (col <= row)
        weights, scale = [], []
        for h in range(2):
            sink = sink_s[h]
            t = [
                jnp.where(same[j], s[h * BLK : (h + 1) * BLK, j * BLK : (j + 1) * BLK], NEG_LARGE)
                for j in range(3)
            ]
            top = jnp.max(jnp.maximum(jnp.maximum(t[0], t[1]), t[2]), axis=-1, keepdims=True)
            top = jnp.maximum(top, sink)
            p = [jnp.exp(v - top) for v in t]
            total = jnp.sum(p[0] + p[1] + p[2], axis=-1, keepdims=True) + jnp.exp(sink - top)
            weights.append(jnp.concatenate(p, axis=1).astype(BF16))
            scale.append(1.0 / total)
        o = dot(jnp.concatenate(weights, axis=0), kvb)
        o0, o1 = o[:BLK] * scale[0], o[BLK:] * scale[1]
        return jnp.where(low, pltpu.roll(o0, 64, 1), o1).astype(BF16)

    def hand_out(blk):
        rows = pl.ds(pl.multiple_of(blk * BLK, BLK), BLK)
        mine = pl.ds(pl.multiple_of(tp * BLK, BLK), BLK)

        @pl.when(blk != tp)
        def _():
            pltpu.make_async_remote_copy(
                src_ref=att_own.at[rows, :], dst_ref=att_all.at[:, mine],
                send_sem=ss.at[a2a + blk], recv_sem=rs.at[a2a + tp],
                device_id=(sp, blk), device_id_type=MESH,
            ).start()

        @pl.when(blk == tp)
        def _():
            att_all[:, mine] = att_own[rows, :]

    @scoped("attend")
    def attend(first, second):
        values = [attended(first), attended(second)]
        for blk, v in zip((first, second), values):
            att_own[pl.ds(pl.multiple_of(blk * BLK, BLK), BLK), :] = v
        for blk in (first, second):
            hand_out(blk)

    def inner(i, carry):
        attend(2 * i + 1, 2 * i + 2)
        return carry

    lax.fori_loop(0, 2, inner, 0)
    for to in (BP, BM):
        pass_on("u", (0, 0), to)
    lax.fori_loop(2, 3, inner, 0)
    for key in ("kv_l", "kv_r", "doc_l", "doc_r"):
        arrive(key)
    docx[pl.ds(0, 8), :] = jnp.where(sp == 0, -1.0, doc_l[...].astype(F32))
    docx[pl.ds(16, 8), :] = jnp.where(sp == 15, -1.0, doc_r[...].astype(F32))

    def outer(i, carry):
        attend(i, i + 7)
        return carry

    lax.fori_loop(0, 1, outer, 0)

    def a2a_copy(i):
        other = (tp + i) % 8
        return pltpu.make_async_remote_copy(
            src_ref=att_own.at[pl.ds(pl.multiple_of(other * BLK, BLK), BLK), :],
            dst_ref=att_all.at[:, pl.ds(pl.multiple_of(other * BLK, BLK), BLK)],
            send_sem=ss.at[a2a + other], recv_sem=rs.at[a2a + other],
            device_id=(sp, other), device_id_type=MESH,
        )

    @scoped("a2a_wait")
    def a2a_wait():
        local["ow"].wait()
        local["st"].wait()
        local["g1"].wait()
        for i in range(1, 8):
            a2a_copy(i).wait_recv()

    need("u", (3, 0))
    need("u", (1, 0))
    a2a_wait()

    def project(n):
        cols = pl.ds(n * 512, 512)
        xbuf[:, cols] = dot(att_all[...], owv[:, cols]) + stv[:, cols].astype(F32)

    @scoped("projection")
    def projection():
        for n in range(4):
            project(n)

    projection()

    def cols_of(rank):
        dy, dz = ORDER[rank]
        return pl.ds(pl.multiple_of((((z + dz) % R) * R + (y + dy) % R) * BLK, BLK), BLK)

    HALF = BLK // 2
    half = lambda h: pl.ds(h * HALF, HALF)

    def fs_send(name, src, dst, h, dev):
        send((name, h), fs.at[src[0], src[1], half(h), :], fs.at[dst[0], dst[1], half(h), :], dev)

    @scoped("first_norm")
    def first_norm(h):
        centre, factor = moments(xbuf[half(h), :])
        for r in range(16):
            c = cols_of(r)
            v = (xbuf[half(h), c] - centre) * factor * g1[:, c]
            fs[0, 0, half(h), pl.ds(r * BLK, BLK)] = v.astype(BF16)

    for h in range(2):
        first_norm(h)
        if h == 0:
            fs_send("x_l", (0, 0), (0, 3), 0, right)
    fs_send("x_r", (0, 0), (0, 1), 1, left)
    fs_send("x_l", (0, 0), (0, 3), 1, right)
    fs_send("x_r", (0, 0), (0, 1), 0, left)
    for h in range(2):
        fs_send("c0", (0, 0), (1, 0), h, partner)

    @scoped("gather_rows")
    def gather_rows(name, h):
        arrive((name, h))
        if name == "x_l":
            if h == 0:
                fs_send("x_2", (0, 3), (0, 2), 0, right)
            fs_send("c3", (0, 3), (1, 3), h, partner)
        elif name == "x_r":
            if h == 1:
                fs_send("x_2", (0, 1), (0, 2), 1, left)
            fs_send("c1", (0, 1), (1, 1), h, partner)
        elif name == "x_2":
            fs_send("c2", (0, 2), (1, 2), h, partner)

    def needs(w, ranks):
        for o in ranks:
            for origin in (o, (o[1], o[0])):
                if origin != (0, 0):
                    need(w, origin)

    @scoped("hidden_a")
    def hidden_a(dx):
        for h in range(2):
            arrive((f"c{dx}", h))
        needs("u", ORDER[: KA // BLK])
        for n in range(HID // 256):
            cols = pl.ds(n * 256, 256)
            rows = fs[:, dx, :, 0:KA].reshape(2 * BLK, KA)
            hacc[min(dx, 2), :, cols] = dot(rows, up_all[0:KA, cols])

    @scoped("hidden")
    def hidden(dx):
        for h in range(2):
            arrive((f"c{dx}", h))
        needs("u", ORDER)
        lo = 0 if dx == 2 else KA
        for n in range(HID // 256):
            cols = pl.ds(n * 256, 256)
            rows = fs[:, dx, :, lo:D].reshape(2 * BLK, D - lo)
            v = dot(rows, up_all[lo:D, cols])
            if lo:
                v = v + hacc[min(dx, 2), :, cols]
            v = jnp.maximum(v, 0.0)
            act[:, dx, :, cols] = (v * v).astype(BF16).reshape(2, BLK, 256)

    @scoped("product_a")
    def product_a(j):
        needs("d", ORDER[2 * j : 2 * j + 2])
        cols = pl.ds(j * CW, CW)
        psend[j] = dot(act[1].reshape(4 * BLK, HID), dn_all[:, cols]).astype(BF16).reshape(R, BLK, CW)
        send(("p", j), psend.at[j], prx.at[j], partner)

    @scoped("product_b")
    def product_b(j):
        cols = pl.ds(j * CW, CW)
        pown[j] = dot(act[0].reshape(4 * BLK, HID), dn_all[:, cols]).reshape(R, BLK, CW)

    @scoped("pair_sum")
    def pair_sum(j):
        arrive(("p", j))
        s2[j] = (pown[j, 2] + prx[j, 2].astype(F32)).astype(BF16)
        send(("mid_l", j), s2.at[j, pl.ds(0, HALF), :], mid_l.at[j], right)
        send(("mid_r", j), s2.at[j, pl.ds(HALF, HALF), :], mid_r.at[j], left)
        macc[:, pl.ds(j * CW, CW)] = pown[j, 0] + prx[j, 0].astype(F32)

    @scoped("middle")
    def middle(j):
        lo, hi = pl.ds(0, HALF), pl.ds(HALF, HALF)
        s1[j, hi, :] = (pown[j, 1, hi, :] + prx[j, 1, hi, :].astype(F32)).astype(BF16)
        s3[j, lo, :] = (pown[j, 3, lo, :] + prx[j, 3, lo, :].astype(F32)).astype(BF16)
        arrive(("mid_l", j))
        s1[j, lo, :] = (pown[j, 1, lo, :] + prx[j, 1, lo, :].astype(F32) + mid_l[j].astype(F32)).astype(BF16)
        send(("fin_l", j), s1.at[j], fin_l.at[j], right)
        arrive(("mid_r", j))
        s3[j, hi, :] = (pown[j, 3, hi, :] + prx[j, 3, hi, :].astype(F32) + mid_r[j].astype(F32)).astype(BF16)
        send(("fin_r", j), s3.at[j], fin_r.at[j], left)

    @scoped("total_sum")
    def total_sum(j):
        arrive(("fin_l", j))
        arrive(("fin_r", j))
        macc[:, pl.ds(j * CW, CW)] += fin_l[j].astype(F32) + fin_r[j].astype(F32)

    need("u", (0, 3))
    need("u", (2, 0))
    need("u", (3, 1))
    need("u", (1, 3))
    need("u", (1, 1))
    hidden_a(0)
    gather_rows("x_l", 0)
    gather_rows("x_r", 1)
    need("u", (2, 1))
    need("u", (2, 3))
    own_down(AP, AM)
    own_down(BP, BM)
    gather_rows("x_l", 1)
    gather_rows("x_r", 0)
    hidden_a(3)
    hidden_a(1)
    hidden(0)
    hidden(1)
    hidden(3)
    gather_rows("x_2", 0)
    gather_rows("x_2", 1)
    need("d", (3, 0))
    need("d", (1, 0))
    hidden(2)
    need("d", (0, 3))
    product_a(0)
    product_b(0)
    product_a(1)
    need("d", (2, 0))
    product_b(1)
    pair_sum(0)
    need("d", (3, 1))
    product_a(2)
    pair_sum(1)
    product_b(2)
    middle(0)
    pair_sum(2)
    need("d", (1, 3))
    need("d", (1, 1))
    product_a(3)
    middle(1)
    product_b(3)
    pair_sum(3)
    total_sum(0)
    need("d", (2, 1))
    product_a(4)
    middle(2)
    product_b(4)
    total_sum(1)
    pair_sum(4)
    middle(3)
    need("d", (2, 3))
    product_a(5)
    product_b(5)
    total_sum(2)
    product_a(6)
    pair_sum(5)
    middle(4)
    product_b(6)
    product_a(7)
    total_sum(3)
    pair_sum(6)
    product_b(7)
    middle(5)
    pair_sum(7)
    total_sum(4)
    middle(6)
    total_sum(5)
    middle(7)
    total_sum(6)
    total_sum(7)
    @scoped("last_norm")
    def last_norm(h):
        macc[half(h), :] += fs[0, 0, half(h), :].astype(F32)
        centre, factor = moments(macc[half(h), :])
        for r in range(16):
            c = cols_of(r)
            v = (macc[half(h), pl.ds(r * BLK, BLK)] - centre) * factor * g2[:, c]
            out[half(h), c] = v.astype(BF16)

    local["g2"].wait()
    for h in range(2):
        last_norm(h)

    @scoped("drain")
    def drain():
        for copy in sent:
            copy.wait_send()
        for i in range(1, 8):
            a2a_copy(i).wait_send()

    drain()


def far(v):
    return pltpu.with_memory_space_constraint(v, pltpu.HBM)


def per_device(q, kv, sink, doc, stream, ow, g1, up, dn, g2):
    vm, anyw = pl.BlockSpec(memory_space=pltpu.VMEM), pl.BlockSpec(memory_space=pl.ANY)
    smem = pl.BlockSpec(memory_space=pltpu.SMEM)
    return pl.pallas_call(
        kernel,
        out_shape=jax.ShapeDtypeStruct(stream.shape, BF16),
        in_specs=[anyw, anyw, smem, anyw, anyw, anyw, anyw, anyw, anyw, anyw],
        out_specs=vm,
        scratch_shapes=[
            pltpu.VMEM((1, D), F32),
            pltpu.VMEM((1, D), F32),
            pltpu.VMEM((1024, BLK), BF16),
            pltpu.VMEM((1024 + 2 * BLK, BLK), BF16),
            pltpu.VMEM((8, BLK), jnp.int32),
            pltpu.VMEM((8, BLK), jnp.int32),
            pltpu.VMEM((8, BLK), jnp.int32),
            pltpu.VMEM((24, BLK), F32),
            pltpu.VMEM((BLK, D), BF16),
            pltpu.VMEM((1024, D), BF16),
            pltpu.VMEM((1024, BLK), BF16),
            pltpu.VMEM((BLK, 1024), BF16),
            pltpu.VMEM((BLK, D), F32),
            pltpu.VMEM((D, HID), BF16),
            pltpu.VMEM((HID, D), BF16),
            pltpu.VMEM((2, R, BLK, D), BF16),
            pltpu.VMEM((3, 2 * BLK, HID), F32),
            pltpu.VMEM((2, R, BLK, HID), BF16),
            pltpu.VMEM((NCH, R, BLK, CW), BF16),
            pltpu.VMEM((NCH, R, BLK, CW), BF16),
            pltpu.VMEM((NCH, R, BLK, CW), F32),
            pltpu.VMEM((NCH, BLK, CW), BF16),
            pltpu.VMEM((NCH, BLK, CW), BF16),
            pltpu.VMEM((NCH, BLK, CW), BF16),
            pltpu.VMEM((NCH, BLK // 2, CW), BF16),
            pltpu.VMEM((NCH, BLK // 2, CW), BF16),
            pltpu.VMEM((NCH, BLK, CW), BF16),
            pltpu.VMEM((NCH, BLK, CW), BF16),
            pltpu.VMEM((BLK, D), F32),
            pltpu.SemaphoreType.DMA((112,)),
            pltpu.SemaphoreType.DMA((112,)),
            pltpu.SemaphoreType.DMA((9,)),
        ],
        compiler_params=pltpu.CompilerParams(
            collective_id=0, has_side_effects=True, vmem_limit_bytes=48 * 1024 * 1024
        ),
        name="layer",
    )(
        far(q), far(kv.reshape(1024, BLK)), far(sink), far(doc.reshape(8, BLK)), far(stream), far(ow),
        far(g1.reshape(1, D)), far(up), far(dn), far(g2.reshape(1, D)),
    )


def solution(mesh):
    placed = (
        P("sp", "tp"),
        P("sp", "tp", None),
        P("tp"),
        P("sp"),
        P(("sp", "tp"), None),
        P(),
        P(),
        P("sp", "tp"),
        P("tp", "sp"),
        P(),
    )
    return jax.shard_map(
        per_device, mesh=mesh, in_specs=placed, out_specs=P(("sp", "tp"), None), check_vma=False
    )
```

```python
import functools

import jax
import jax.numpy as jnp
from jax import lax
from jax.experimental import pallas as pl
from jax.experimental.pallas import tpu as pltpu
from jax.sharding import PartitionSpec as P

MESH = pl.DeviceIdType.MESH
F32 = jnp.float32
BF16 = jnp.bfloat16
NEG_LARGE = -1e30
NORM_EPS = 1e-05
R = 4
BLK = 128
D = 2048
HID = 1024
NCH = 8
CW = D // NCH

ORDER = [
    (0, 0), (1, 0), (3, 0), (0, 1), (0, 3), (3, 3), (3, 1), (1, 1),
    (1, 3), (2, 0), (0, 2), (3, 2), (2, 3), (2, 1), (1, 2), (2, 2),
]
RANK = {o: i for i, o in enumerate(ORDER)}

AP, AM, BP, BM = (1, 0), (-1, 0), (0, 1), (0, -1)
ONWARD = {
    (3, 0): [(AP, 0), (BP, None), (BM, None)],
    (1, 0): [(AM, 1), (BP, None), (BM, None)],
    (2, 0): [(BP, None), (BM, None)],
    (0, 3): [(BP, 0)],
    (0, 1): [(BM, 1)],
    (3, 3): [(BP, None)],
    (1, 1): [(BM, None)],
    (2, 3): [(BP, 0)],
    (2, 1): [(BM, 1)],
}
HALVED = ((2, 0), (0, 2), (2, 2))
KA = HID


def nt_dot(a, b):
    return lax.dot_general(a, b, (((1,), (1,)), ((), ())), preferred_element_type=F32)


def dot(a, b):
    return jnp.dot(a, b, preferred_element_type=F32)


def moments(x):
    centre = jnp.mean(x, axis=-1, keepdims=True)
    shifted = x - centre
    return centre, lax.rsqrt(jnp.mean(shifted * shifted, axis=-1, keepdims=True) + NORM_EPS)


def scoped(name):
    def wrap(f):
        @functools.wraps(f)
        def run(*args):
            tag = "_".join("".join(c for c in str(v) if c.isalnum()) for v in args if isinstance(v, (int, str, tuple)))
            with jax.named_scope(f"{name}#v={tag}"):
                return f(*args)

        return run

    return wrap


class Sems:
    def __init__(self):
        self.index = {}

    def at(self, key, count=1):
        if key not in self.index:
            self.index[key] = (sum(c for _, c in self.index.values()), count)
        return self.index[key][0]


def kernel(
    q_h, kv_h, sink_s, doc_h, st_h, ow_h, g1_h, up_h, dn_h, g2_h, out,
    g1, g2, qv, kvx, docv, doc_l, doc_r, docx, stv, owv, att_own, att_all, xbuf,
    up_all, dn_all, fs, hacc, act, psend, prx, pown, s1, s2, s3, mid_l, mid_r, fin_l, fin_r, macc,
    ss, rs, ls,
):
    sp, tp = lax.axis_index("sp"), lax.axis_index("tp")
    z, y = sp // R, sp % R
    x, core = tp // 2, tp % 2
    stride_a, stride_b = 1 + 3 * core, 4 - 3 * core
    a = y * (1 - core) + z * core
    b = z * (1 - core) + y * core

    def sp_of(da, db):
        return ((a + da) % R) * stride_a + ((b + db) % R) * stride_b

    partner = (sp, x * 2 + (1 - core))
    right = (sp, ((x + 1) % R) * 2 + core)
    left = (sp, ((x + R - 1) % R) * 2 + core)
    sp_next, sp_prev = (sp + 1) % 16, (sp + 15) % 16

    barrier = pltpu.get_barrier_semaphore()
    greet = [(sp, (tp + i) % 8) for i in range(1, 8)]
    greet += [(sp_of(da, db), tp) for da, db in ((1, 0), (3, 0), (0, 1), (0, 3))]
    greet += [(sp_next, tp), (sp_prev, tp)]
    for dev in greet:
        pl.semaphore_signal(barrier, inc=1, device_id=dev, device_id_type=MESH)
    local_names = ["kv", "doc", "up", "q", "st", "ow", "dn", "g1", "g2"]
    pairs = {
        "kv": (kv_h, kvx.at[pl.ds(BLK, 1024), :]),
        "doc": (doc_h, docv),
        "q": (q_h, qv),
        "up": (up_h, up_all.at[pl.ds(0, BLK), :]),
        "dn": (dn_h, dn_all.at[:, pl.ds(0, BLK)]),
        "st": (st_h, stv),
        "ow": (ow_h, owv),
        "g1": (g1_h, g1),
        "g2": (g2_h, g2),
    }
    local = {n: pltpu.make_async_copy(*pairs[n], ls.at[i]) for i, n in enumerate(local_names)}
    for n in local_names:
        local[n].start()

    pl.semaphore_wait(barrier, len(greet))

    sems = Sems()
    sent = []
    waited = set()
    arriving = {}

    def send(key, src, dst, dev):
        i = sems.at(key)
        copy = pltpu.make_async_remote_copy(
            src_ref=src, dst_ref=dst, send_sem=ss.at[i], recv_sem=rs.at[i], device_id=dev, device_id_type=MESH
        )
        copy.start()
        sent.append(copy)
        arriving[key] = copy

    def arrive(key):
        if key not in waited:
            waited.add(key)
            arriving[key].wait_recv()

    local["kv"].wait()
    local["doc"].wait()
    send("kv_l", kvx.at[pl.ds(1024, BLK), :], kvx.at[pl.ds(0, BLK), :], (sp_next, tp))
    send("kv_r", kvx.at[pl.ds(BLK, BLK), :], kvx.at[pl.ds(1024 + BLK, BLK), :], (sp_prev, tp))
    send("doc_l", docv, doc_l, (sp_next, tp))
    send("doc_r", docv, doc_r, (sp_prev, tp))

    def block(w, origin, at, half):
        ra, rb = (origin[0] - at[0]) % R, (origin[1] - at[1]) % R
        r0, r1 = RANK[(ra, rb)], RANK[(rb, ra)]
        slot = (r0 + core * (r1 - r0)) * BLK
        size = BLK if w == "u" else HID
        lo, n = {None: (0, size), 0: (0, size // 2), 1: (size // 2, size // 2)}[half]
        if w == "u":
            return up_all.at[pl.ds(pl.multiple_of(slot + lo, BLK // 2), n), :]
        return dn_all.at[pl.ds(lo, n), pl.ds(pl.multiple_of(slot, BLK), BLK)]

    def pass_on(w, origin, to, half=None):
        rel = ((origin[0] - to[0]) % R, (origin[1] - to[1]) % R)
        send(
            (w, rel, half), block(w, origin, (0, 0), half), block(w, origin, to, half),
            (sp_of(to[0] % R, to[1] % R), tp),
        )

    relayed = set()

    @scoped("need")
    def need(w, origin):
        if (w, origin) in relayed:
            return
        relayed.add((w, origin))
        for h in (0, 1) if origin in HALVED else (None,):
            arrive((w, origin, h))
        for to, h in ONWARD.get(origin, ()):
            pass_on(w, origin, to, h)

    def own_down(*ways):
        for to in ways:
            pass_on("d", (0, 0), to)

    local["up"].wait()
    for to in (AP, AM):
        pass_on("u", (0, 0), to)
    local["dn"].wait()
    own_down(AP, AM)

    local["q"].wait()
    docx[pl.ds(8, 8), :] = docv[...].astype(F32)
    row = lax.broadcasted_iota(jnp.int32, (BLK, BLK), 0)
    col = lax.broadcasted_iota(jnp.int32, (BLK, BLK), 1)
    low = col < 64
    a2a = sems.at("a2a", 8)

    def attended(blk):
        rows = pl.ds(pl.multiple_of(blk * BLK, BLK), BLK)
        qf = qv[rows, :].astype(F32) * 0.125
        q2 = jnp.concatenate(
            [jnp.where(low, qf, 0.0), jnp.where(low, pltpu.roll(qf, 64, 1), 0.0)], axis=0
        ).astype(BF16)
        kvb = kvx[pl.ds(pl.multiple_of(blk * BLK, BLK), 3 * BLK), :]
        s = nt_dot(q2, kvb)
        dq = jnp.broadcast_to(docx[pl.ds(blk + 8, 1), :], (BLK, BLK)).T
        same = [jnp.broadcast_to(docx[pl.ds(blk + 7 + j, 1), :], (BLK, BLK)) == dq for j in range(3)]
        same[0] = same[0] & (col >= row)
        same[2] = same[2] & (col <= row)
        weights, scale = [], []
        for h in range(2):
            sink = sink_s[h]
            t = [
                jnp.where(same[j], s[h * BLK : (h + 1) * BLK, j * BLK : (j + 1) * BLK], NEG_LARGE)
                for j in range(3)
            ]
            top = jnp.max(jnp.maximum(jnp.maximum(t[0], t[1]), t[2]), axis=-1, keepdims=True)
            top = jnp.maximum(top, sink)
            p = [jnp.exp(v - top) for v in t]
            total = jnp.sum(p[0] + p[1] + p[2], axis=-1, keepdims=True) + jnp.exp(sink - top)
            weights.append(jnp.concatenate(p, axis=1).astype(BF16))
            scale.append(1.0 / total)
        o = dot(jnp.concatenate(weights, axis=0), kvb)
        o0, o1 = o[:BLK] * scale[0], o[BLK:] * scale[1]
        return jnp.where(low, pltpu.roll(o0, 64, 1), o1).astype(BF16)

    def hand_out(blk):
        rows = pl.ds(pl.multiple_of(blk * BLK, BLK), BLK)
        mine = pl.ds(pl.multiple_of(tp * BLK, BLK), BLK)

        @pl.when(blk != tp)
        def _():
            pltpu.make_async_remote_copy(
                src_ref=att_own.at[rows, :], dst_ref=att_all.at[:, mine],
                send_sem=ss.at[a2a + blk], recv_sem=rs.at[a2a + tp],
                device_id=(sp, blk), device_id_type=MESH,
            ).start()

        @pl.when(blk == tp)
        def _():
            att_all[:, mine] = att_own[rows, :]

    @scoped("attend")
    def attend(first, second):
        values = [attended(first), attended(second)]
        for blk, v in zip((first, second), values):
            att_own[pl.ds(pl.multiple_of(blk * BLK, BLK), BLK), :] = v
        for blk in (first, second):
            hand_out(blk)

    def inner(i, carry):
        attend(2 * i + 1, 2 * i + 2)
        return carry

    lax.fori_loop(0, 2, inner, 0)
    for to in (BP, BM):
        pass_on("u", (0, 0), to)
    lax.fori_loop(2, 3, inner, 0)
    for key in ("kv_l", "kv_r", "doc_l", "doc_r"):
        arrive(key)
    docx[pl.ds(0, 8), :] = jnp.where(sp == 0, -1.0, doc_l[...].astype(F32))
    docx[pl.ds(16, 8), :] = jnp.where(sp == 15, -1.0, doc_r[...].astype(F32))

    def outer(i, carry):
        attend(i, i + 7)
        return carry

    lax.fori_loop(0, 1, outer, 0)

    def a2a_copy(i):
        other = (tp + i) % 8
        return pltpu.make_async_remote_copy(
            src_ref=att_own.at[pl.ds(pl.multiple_of(other * BLK, BLK), BLK), :],
            dst_ref=att_all.at[:, pl.ds(pl.multiple_of(other * BLK, BLK), BLK)],
            send_sem=ss.at[a2a + other], recv_sem=rs.at[a2a + other],
            device_id=(sp, other), device_id_type=MESH,
        )

    @scoped("a2a_wait")
    def a2a_wait():
        local["ow"].wait()
        local["st"].wait()
        local["g1"].wait()
        for i in range(1, 8):
            a2a_copy(i).wait_recv()

    a2a_wait()

    def project(n):
        cols = pl.ds(n * 512, 512)
        xbuf[:, cols] = dot(att_all[...], owv[:, cols]) + stv[:, cols].astype(F32)

    @scoped("projection")
    def projection():
        for n in range(4):
            project(n)

    projection()

    def cols_of(rank):
        dy, dz = ORDER[rank]
        return pl.ds(pl.multiple_of((((z + dz) % R) * R + (y + dy) % R) * BLK, BLK), BLK)

    HALF = BLK // 2
    half = lambda h: pl.ds(h * HALF, HALF)

    def fs_send(name, src, dst, i, dev, n=HALF):
        rows = pl.ds(i * n, n)
        send((name, i), fs.at[src[0], src[1], rows, :], fs.at[dst[0], dst[1], rows, :], dev)

    @scoped("first_norm")
    def first_norm(h):
        centre, factor = moments(xbuf[half(h), :])
        for r in range(16):
            c = cols_of(r)
            v = (xbuf[half(h), c] - centre) * factor * g1[:, c]
            fs[0, 0, half(h), pl.ds(r * BLK, BLK)] = v.astype(BF16)

    for h in range(2):
        first_norm(h)
        if h == 0:
            fs_send("x_l", (0, 0), (0, 3), 0, right)
    fs_send("x_r", (0, 0), (0, 1), 1, left)
    fs_send("x_l", (0, 0), (0, 3), 1, right)
    fs_send("x_r", (0, 0), (0, 1), 0, left)
    for h in range(2):
        fs_send("c0", (0, 0), (1, 0), h, partner)

    @scoped("gather_rows")
    def gather_rows(name, h):
        arrive((name, h))
        if name == "x_2":
            fs_send("c2", (0, 2), (1, 2), h, partner, BLK // 4)
            return
        slot, onward, first = (3, right, 0) if name == "x_l" else (1, left, 1)
        if h == first:
            for q in (2 * h, 2 * h + 1):
                fs_send("x_2", (0, slot), (0, 2), q, onward, BLK // 4)
        fs_send(f"c{slot}", (0, slot), (1, slot), h, partner)

    def needs(w, ranks):
        for o in ranks:
            for origin in (o, (o[1], o[0])):
                if origin != (0, 0):
                    need(w, origin)

    @scoped("hidden_a")
    def hidden_a(dx):
        for h in range(2):
            arrive((f"c{dx}", h))
        needs("u", ORDER[: KA // BLK])
        for n in range(HID // 256):
            cols = pl.ds(n * 256, 256)
            rows = fs[:, dx, :, 0:KA].reshape(2 * BLK, KA)
            hacc[min(dx, 2), :, cols] = dot(rows, up_all[0:KA, cols])

    @scoped("hidden")
    def hidden(dx):
        for i in range(4 if dx == 2 else 2):
            arrive((f"c{dx}", i))
        needs("u", ORDER)
        lo = 0 if dx == 2 else KA
        for n in range(HID // 256):
            cols = pl.ds(n * 256, 256)
            rows = fs[:, dx, :, lo:D].reshape(2 * BLK, D - lo)
            v = dot(rows, up_all[lo:D, cols])
            if lo:
                v = v + hacc[min(dx, 2), :, cols]
            v = jnp.maximum(v, 0.0)
            act[:, dx, :, cols] = (v * v).astype(BF16).reshape(2, BLK, 256)

    @scoped("product_a")
    def product_a(j):
        needs("d", ORDER[2 * j : 2 * j + 2])
        cols = pl.ds(j * CW, CW)
        psend[j] = dot(act[1].reshape(4 * BLK, HID), dn_all[:, cols]).astype(BF16).reshape(R, BLK, CW)
        send(("p", j), psend.at[j], prx.at[j], partner)

    @scoped("product_b")
    def product_b(j):
        cols = pl.ds(j * CW, CW)
        pown[j] = dot(act[0].reshape(4 * BLK, HID), dn_all[:, cols]).reshape(R, BLK, CW)

    LO, HI = pl.ds(0, HALF), pl.ds(HALF, HALF)

    def pair(j, dx, rows=slice(None)):
        return pown[j, dx, rows, :] + prx[j, dx, rows, :].astype(F32)

    @scoped("pair_sum")
    def pair_sum(j):
        arrive(("p", j))
        s2[j] = pair(j, 2).astype(BF16)
        send(("mid_l", j), s2.at[j, LO, :], mid_l.at[j], right)
        send(("mid_r", j), s2.at[j, HI, :], mid_r.at[j], left)
        s1[j, HI, :] = pair(j, 1, HI).astype(BF16)
        s3[j, LO, :] = pair(j, 3, LO).astype(BF16)
        send(("dir_l", j), s1.at[j, HI, :], fin_l.at[j, HI, :], right)
        send(("dir_r", j), s3.at[j, LO, :], fin_r.at[j, LO, :], left)
        macc[:, pl.ds(j * CW, CW)] = pair(j, 0)

    @scoped("middle")
    def middle(j):
        arrive(("mid_l", j))
        s1[j, LO, :] = (pair(j, 1, LO) + mid_l[j].astype(F32)).astype(BF16)
        send(("fin_l", j), s1.at[j, LO, :], fin_l.at[j, LO, :], right)
        arrive(("mid_r", j))
        s3[j, HI, :] = (pair(j, 3, HI) + mid_r[j].astype(F32)).astype(BF16)
        send(("fin_r", j), s3.at[j, HI, :], fin_r.at[j, HI, :], left)

    @scoped("total_sum")
    def total_sum(j):
        for name in ("dir_l", "dir_r", "fin_l", "fin_r"):
            arrive((name, j))
        macc[:, pl.ds(j * CW, CW)] += fin_l[j].astype(F32) + fin_r[j].astype(F32)

    need("u", (3, 0))
    need("u", (1, 0))
    need("u", (0, 3))
    need("u", (0, 1))
    need("u", (2, 0))
    need("u", (3, 3))
    gather_rows("x_l", 0)
    gather_rows("x_r", 1)
    need("u", (1, 1))
    hidden_a(0)
    gather_rows("x_l", 1)
    gather_rows("x_r", 0)
    need("u", (2, 3))
    need("u", (2, 1))
    own_down(BP, BM)
    need("d", (3, 0))
    need("d", (1, 0))
    hidden_a(3)
    hidden_a(1)
    gather_rows("x_2", 0)
    gather_rows("x_2", 2)
    need("d", (2, 0))
    gather_rows("x_2", 1)
    gather_rows("x_2", 3)
    hidden(0)
    hidden(1)
    hidden(3)
    hidden(2)
    need("d", (0, 3))
    need("d", (0, 1))
    product_a(0)
    product_b(0)
    product_a(1)
    need("d", (3, 3))
    product_b(1)
    pair_sum(0)
    product_a(2)
    product_b(2)
    pair_sum(1)
    need("d", (1, 1))
    product_a(3)
    pair_sum(2)
    middle(0)
    product_b(3)
    middle(1)
    pair_sum(3)
    need("d", (2, 3))
    need("d", (2, 1))
    middle(2)
    product_a(4)
    total_sum(0)
    product_b(4)
    total_sum(1)
    middle(3)
    pair_sum(4)
    product_a(5)
    total_sum(2)
    product_b(5)
    product_a(6)
    total_sum(3)
    product_b(6)
    pair_sum(5)
    middle(4)
    product_a(7)
    pair_sum(6)
    product_b(7)
    pair_sum(7)
    middle(5)
    total_sum(4)
    middle(6)
    middle(7)
    total_sum(5)
    total_sum(6)
    total_sum(7)
    @scoped("last_norm")
    def last_norm(h):
        macc[half(h), :] += fs[0, 0, half(h), :].astype(F32)
        centre, factor = moments(macc[half(h), :])
        for r in range(16):
            c = cols_of(r)
            v = (macc[half(h), pl.ds(r * BLK, BLK)] - centre) * factor * g2[:, c]
            out[half(h), c] = v.astype(BF16)

    local["g2"].wait()
    for h in range(2):
        last_norm(h)

    @scoped("drain")
    def drain():
        for copy in sent:
            copy.wait_send()
        for i in range(1, 8):
            a2a_copy(i).wait_send()

    drain()


def far(v):
    return pltpu.with_memory_space_constraint(v, pltpu.HBM)


def per_device(q, kv, sink, doc, stream, ow, g1, up, dn, g2):
    vm, anyw = pl.BlockSpec(memory_space=pltpu.VMEM), pl.BlockSpec(memory_space=pl.ANY)
    smem = pl.BlockSpec(memory_space=pltpu.SMEM)
    return pl.pallas_call(
        kernel,
        out_shape=jax.ShapeDtypeStruct(stream.shape, BF16),
        in_specs=[anyw, anyw, smem, anyw, anyw, anyw, anyw, anyw, anyw, anyw],
        out_specs=vm,
        scratch_shapes=[
            pltpu.VMEM((1, D), F32),
            pltpu.VMEM((1, D), F32),
            pltpu.VMEM((1024, BLK), BF16),
            pltpu.VMEM((1024 + 2 * BLK, BLK), BF16),
            pltpu.VMEM((8, BLK), jnp.int32),
            pltpu.VMEM((8, BLK), jnp.int32),
            pltpu.VMEM((8, BLK), jnp.int32),
            pltpu.VMEM((24, BLK), F32),
            pltpu.VMEM((BLK, D), BF16),
            pltpu.VMEM((1024, D), BF16),
            pltpu.VMEM((1024, BLK), BF16),
            pltpu.VMEM((BLK, 1024), BF16),
            pltpu.VMEM((BLK, D), F32),
            pltpu.VMEM((D, HID), BF16),
            pltpu.VMEM((HID, D), BF16),
            pltpu.VMEM((2, R, BLK, D), BF16),
            pltpu.VMEM((3, 2 * BLK, HID), F32),
            pltpu.VMEM((2, R, BLK, HID), BF16),
            pltpu.VMEM((NCH, R, BLK, CW), BF16),
            pltpu.VMEM((NCH, R, BLK, CW), BF16),
            pltpu.VMEM((NCH, R, BLK, CW), F32),
            pltpu.VMEM((NCH, BLK, CW), BF16),
            pltpu.VMEM((NCH, BLK, CW), BF16),
            pltpu.VMEM((NCH, BLK, CW), BF16),
            pltpu.VMEM((NCH, BLK // 2, CW), BF16),
            pltpu.VMEM((NCH, BLK // 2, CW), BF16),
            pltpu.VMEM((NCH, BLK, CW), BF16),
            pltpu.VMEM((NCH, BLK, CW), BF16),
            pltpu.VMEM((BLK, D), F32),
            pltpu.SemaphoreType.DMA((128,)),
            pltpu.SemaphoreType.DMA((128,)),
            pltpu.SemaphoreType.DMA((9,)),
        ],
        compiler_params=pltpu.CompilerParams(
            collective_id=0, has_side_effects=True, vmem_limit_bytes=48 * 1024 * 1024
        ),
        name="layer",
    )(
        far(q), far(kv.reshape(1024, BLK)), far(sink), far(doc.reshape(8, BLK)), far(stream), far(ow),
        far(g1.reshape(1, D)), far(up), far(dn), far(g2.reshape(1, D)),
    )


def solution(mesh):
    placed = (
        P("sp", "tp"),
        P("sp", "tp", None),
        P("tp"),
        P("sp"),
        P(("sp", "tp"), None),
        P(),
        P(),
        P("sp", "tp"),
        P("tp", "sp"),
        P(),
    )
    return jax.shard_map(
        per_device, mesh=mesh, in_specs=placed, out_specs=P(("sp", "tp"), None), check_vma=False
    )
```

```python
import functools

import jax
import jax.numpy as jnp
from jax import lax
from jax.experimental import pallas as pl
from jax.experimental.pallas import tpu as pltpu
from jax.sharding import PartitionSpec as P

MESH = pl.DeviceIdType.MESH
F32 = jnp.float32
BF16 = jnp.bfloat16
NEG_LARGE = -1e30
NORM_EPS = 1e-05
R = 4
BLK = 128
D = 2048
HID = 1024
NCH = 8
CW = D // NCH
SENDS, ARRIVALS = 13, 65

ORDER = [
    (0, 0), (1, 0), (3, 0), (0, 1), (0, 3), (3, 3), (3, 1), (1, 1),
    (1, 3), (2, 0), (0, 2), (3, 2), (2, 3), (2, 1), (1, 2), (2, 2),
]
RANK = {o: i for i, o in enumerate(ORDER)}

AP, AM, BP, BM = (1, 0), (-1, 0), (0, 1), (0, -1)
ONWARD = {
    (3, 0): [(AP, 0), (BP, None), (BM, None)],
    (1, 0): [(AM, 1), (BP, None), (BM, None)],
    (2, 0): [(BP, None), (BM, None)],
    (0, 3): [(BP, 0)],
    (0, 1): [(BM, 1)],
    (3, 3): [(BP, None)],
    (1, 1): [(BM, None)],
    (2, 3): [(BP, 0)],
    (2, 1): [(BM, 1)],
}
TOGETHER = (((3, 1), (1, 3)), ((0, 2), (3, 2), (1, 2), (2, 2)))
KA = HID


def nt_dot(a, b):
    return lax.dot_general(a, b, (((1,), (1,)), ((), ())), preferred_element_type=F32)


def dot(a, b):
    return jnp.dot(a, b, preferred_element_type=F32)


def moments(x):
    centre = jnp.mean(x, axis=-1, keepdims=True)
    shifted = x - centre
    return centre, lax.rsqrt(jnp.mean(shifted * shifted, axis=-1, keepdims=True) + NORM_EPS)


def scoped(name):
    def wrap(f):
        @functools.wraps(f)
        def run(*args):
            tag = "_".join("".join(c for c in str(v) if c.isalnum()) for v in args if isinstance(v, (int, str, tuple)))
            with jax.named_scope(f"{name}#v={tag}"):
                return f(*args)

        return run

    return wrap


class Sems:
    def __init__(self):
        self.index = {}

    def at(self, key):
        return self.index.setdefault(key, len(self.index))


def kernel(
    q_h, kv_h, sink_s, doc_h, st_h, ow_h, g1_h, up_h, dn_h, g2_h, out,
    g1, g2, qv, kvx, docv, doc_lr, docx, stv, owv, att_own, att_all, xbuf,
    up_all, dn_all, fs, hacc, act, psend, prx, pown, s1, s2, s3, mid, fin, macc,
    ss, rs, ls,
):
    sp, tp = lax.axis_index("sp"), lax.axis_index("tp")
    z, y = sp // R, sp % R
    x, core = tp // 2, tp % 2
    stride_a, stride_b = 1 + 3 * core, 4 - 3 * core
    a = y * (1 - core) + z * core
    b = z * (1 - core) + y * core

    def sp_of(da, db):
        return ((a + da) % R) * stride_a + ((b + db) % R) * stride_b

    partner = (sp, x * 2 + (1 - core))
    right = (sp, ((x + 1) % R) * 2 + core)
    left = (sp, ((x + R - 1) % R) * 2 + core)
    sp_next, sp_prev = (sp + 1) % 16, (sp + 15) % 16

    barrier = pltpu.get_barrier_semaphore()
    greet = [(sp, (tp + i) % 8) for i in range(1, 8)]
    greet += [(sp_of(da, db), tp) for da, db in ((1, 0), (3, 0), (0, 1), (0, 3))]
    greet += [(sp_next, tp), (sp_prev, tp)]
    for dev in greet:
        pl.semaphore_signal(barrier, inc=1, device_id=dev, device_id_type=MESH)
    local_names = ["kv", "doc", "up", "q", "st", "ow", "dn", "g1", "g2"]
    pairs = {
        "kv": (kv_h, kvx.at[pl.ds(BLK, 1024), :]),
        "doc": (doc_h, docv),
        "q": (q_h, qv),
        "up": (up_h, up_all.at[pl.ds(0, BLK), :]),
        "dn": (dn_h, dn_all.at[:, pl.ds(0, BLK)]),
        "st": (st_h, stv),
        "ow": (ow_h, owv),
        "g1": (g1_h, g1),
        "g2": (g2_h, g2),
    }
    local = {n: pltpu.make_async_copy(*pairs[n], ls.at[i]) for i, n in enumerate(local_names)}
    for n in local_names:
        local[n].start()

    pl.semaphore_wait(barrier, len(greet))

    send_sems, recv_sems = Sems(), Sems()
    ends = {}
    waited = set()

    def send(key, src, dst, dev, group, whole, with_key=None, with_dst=None):
        pltpu.make_async_remote_copy(
            src_ref=src, dst_ref=dst, send_sem=ss.at[send_sems.at(group)],
            recv_sem=rs.at[recv_sems.at(with_key or key)], device_id=dev, device_id_type=MESH,
        ).start()
        ends[("s", group)] = whole
        ends[("r", with_key or key)] = dst if with_dst is None else with_dst

    def wait(kind, key):
        ref = ends[(kind, key)]
        i = (send_sems if kind == "s" else recv_sems).at(key)
        copy = pltpu.make_async_remote_copy(
            src_ref=ref, dst_ref=ref, send_sem=ss.at[i], recv_sem=rs.at[i], device_id=partner, device_id_type=MESH
        )
        copy.wait_send() if kind == "s" else copy.wait_recv()

    def arrive(key):
        if key not in waited:
            waited.add(key)
            wait("r", key)

    local["kv"].wait()
    local["doc"].wait()
    rim = kvx.at[pl.ds(0, 2 * BLK), :]
    for src, dst, dev in ((1024, 0, sp_next), (BLK, 1024 + BLK, sp_prev)):
        rows = kvx.at[pl.ds(src, BLK), :], kvx.at[pl.ds(dst, BLK), :]
        send("kv", *rows, (dev, tp), "kv", rim, "kv", rim)
    send("doc", docv, doc_lr.at[pl.ds(0, 8), :], (sp_next, tp), "doc", doc_lr, "doc", doc_lr)
    send("doc", docv, doc_lr.at[pl.ds(8, 8), :], (sp_prev, tp), "doc", doc_lr, "doc", doc_lr)

    def block(w, origin, at, half):
        ra, rb = (origin[0] - at[0]) % R, (origin[1] - at[1]) % R
        r0, r1 = RANK[(ra, rb)], RANK[(rb, ra)]
        slot = (r0 + core * (r1 - r0)) * BLK
        size = BLK if w == "u" else HID
        lo, n = {None: (0, size), 0: (0, size // 2), 1: (size // 2, size // 2)}[half]
        if w == "u":
            return up_all.at[pl.ds(pl.multiple_of(slot + lo, BLK // 2), n), :]
        return dn_all.at[pl.ds(lo, n), pl.ds(pl.multiple_of(slot, BLK), BLK)]

    def pass_on(w, origin, to, half=None):
        rel = ((origin[0] - to[0]) % R, (origin[1] - to[1]) % R)
        held = up_all if w == "u" else dn_all
        together = {o: g for g in TOGETHER for o in g}.get(rel, (rel,)) if w == "u" else (rel,)
        n = len(together) * BLK
        send(
            (w, rel), block(w, origin, (0, 0), half), block(w, origin, to, half),
            (sp_of(to[0] % R, to[1] % R), tp),
            w, held.at[pl.ds(0, 15 * BLK), :] if w == "u" else held.at[:, pl.ds(0, 15 * BLK)],
            (w, together), held.at[pl.ds(0, n), :] if w == "u" else held.at[:, pl.ds(0, n)],
        )

    relayed = set()

    @scoped("need")
    def need(w, origin):
        if (w, origin) in relayed:
            return
        relayed.add((w, origin))
        arrive((w, {o: g for g in TOGETHER for o in g}.get(origin, (origin,)) if w == "u" else (origin,)))
        for to, h in ONWARD.get(origin, ()):
            pass_on(w, origin, to, h)

    def own_down(*ways):
        for to in ways:
            pass_on("d", (0, 0), to)

    local["up"].wait()
    for to in (AP, AM):
        pass_on("u", (0, 0), to)
    local["dn"].wait()
    own_down(AP, AM)

    local["q"].wait()
    docx[pl.ds(8, 8), :] = docv[...].astype(F32)
    row = lax.broadcasted_iota(jnp.int32, (BLK, BLK), 0)
    col = lax.broadcasted_iota(jnp.int32, (BLK, BLK), 1)
    low = col < 64
    a2a_send, a2a_recv = send_sems.at("a2a"), recv_sems.at("a2a")
    ends[("s", "a2a")] = ends[("r", "a2a")] = att_own.at[pl.ds(0, 7 * BLK), :]

    def attended(blk):
        rows = pl.ds(pl.multiple_of(blk * BLK, BLK), BLK)
        qf = qv[rows, :].astype(F32) * 0.125
        q2 = jnp.concatenate(
            [jnp.where(low, qf, 0.0), jnp.where(low, pltpu.roll(qf, 64, 1), 0.0)], axis=0
        ).astype(BF16)
        kvb = kvx[pl.ds(pl.multiple_of(blk * BLK, BLK), 3 * BLK), :]
        s = nt_dot(q2, kvb)
        dq = jnp.broadcast_to(docx[pl.ds(blk + 8, 1), :], (BLK, BLK)).T
        same = [jnp.broadcast_to(docx[pl.ds(blk + 7 + j, 1), :], (BLK, BLK)) == dq for j in range(3)]
        same[0] = same[0] & (col >= row)
        same[2] = same[2] & (col <= row)
        weights, scale = [], []
        for h in range(2):
            sink = sink_s[h]
            t = [
                jnp.where(same[j], s[h * BLK : (h + 1) * BLK, j * BLK : (j + 1) * BLK], NEG_LARGE)
                for j in range(3)
            ]
            top = jnp.max(jnp.maximum(jnp.maximum(t[0], t[1]), t[2]), axis=-1, keepdims=True)
            top = jnp.maximum(top, sink)
            p = [jnp.exp(v - top) for v in t]
            total = jnp.sum(p[0] + p[1] + p[2], axis=-1, keepdims=True) + jnp.exp(sink - top)
            weights.append(jnp.concatenate(p, axis=1).astype(BF16))
            scale.append(1.0 / total)
        o = dot(jnp.concatenate(weights, axis=0), kvb)
        o0, o1 = o[:BLK] * scale[0], o[BLK:] * scale[1]
        return jnp.where(low, pltpu.roll(o0, 64, 1), o1).astype(BF16)

    def hand_out(blk):
        rows = pl.ds(pl.multiple_of(blk * BLK, BLK), BLK)
        mine = pl.ds(pl.multiple_of(tp * BLK, BLK), BLK)

        @pl.when(blk != tp)
        def _():
            pltpu.make_async_remote_copy(
                src_ref=att_own.at[rows, :], dst_ref=att_all.at[:, mine],
                send_sem=ss.at[a2a_send], recv_sem=rs.at[a2a_recv],
                device_id=(sp, blk), device_id_type=MESH,
            ).start()

        @pl.when(blk == tp)
        def _():
            att_all[:, mine] = att_own[rows, :]

    @scoped("attend")
    def attend(first, second):
        values = [attended(first), attended(second)]
        for blk, v in zip((first, second), values):
            att_own[pl.ds(pl.multiple_of(blk * BLK, BLK), BLK), :] = v
        for blk in (first, second):
            hand_out(blk)

    def inner(i, carry):
        attend(2 * i + 1, 2 * i + 2)
        return carry

    lax.fori_loop(0, 2, inner, 0)
    for to in (BP, BM):
        pass_on("u", (0, 0), to)
    lax.fori_loop(2, 3, inner, 0)
    arrive("kv")
    arrive("doc")
    docx[pl.ds(0, 8), :] = jnp.where(sp == 0, -1.0, doc_lr[pl.ds(0, 8), :].astype(F32))
    docx[pl.ds(16, 8), :] = jnp.where(sp == 15, -1.0, doc_lr[pl.ds(8, 8), :].astype(F32))

    def outer(i, carry):
        attend(i, i + 7)
        return carry

    lax.fori_loop(0, 1, outer, 0)

    @scoped("a2a_wait")
    def a2a_wait():
        local["ow"].wait()
        local["st"].wait()
        local["g1"].wait()
        arrive("a2a")

    a2a_wait()
    need("u", (3, 0))
    need("u", (1, 0))

    def project(n):
        cols = pl.ds(n * 512, 512)
        xbuf[:, cols] = dot(att_all[...], owv[:, cols]) + stv[:, cols].astype(F32)

    @scoped("projection")
    def projection():
        for n in range(4):
            project(n)

    projection()

    def cols_of(rank):
        dy, dz = ORDER[rank]
        return pl.ds(pl.multiple_of((((z + dz) % R) * R + (y + dy) % R) * BLK, BLK), BLK)

    HALF = BLK // 2
    half = lambda h: pl.ds(h * HALF, HALF)

    def fs_send(name, src, dst, i, dev, n=HALF):
        rows = pl.ds(i * n, n)
        to_partner = name[0] == "c"
        send(
            (name, i), fs.at[src[0], src[1], rows, :], fs.at[dst[0], dst[1], rows, :], dev,
            "c" if to_partner else name, fs.at[0] if to_partner else fs.at[0, 0],
            name if to_partner else None, fs.at[1, dst[1]] if to_partner else None,
        )

    @scoped("first_norm")
    def first_norm(h):
        centre, factor = moments(xbuf[half(h), :])
        for r in range(16):
            c = cols_of(r)
            v = (xbuf[half(h), c] - centre) * factor * g1[:, c]
            fs[0, 0, half(h), pl.ds(r * BLK, BLK)] = v.astype(BF16)

    for h in range(2):
        first_norm(h)
        if h == 0:
            fs_send("x_l", (0, 0), (0, 3), 0, right)
    fs_send("x_r", (0, 0), (0, 1), 1, left)
    fs_send("x_l", (0, 0), (0, 3), 1, right)
    fs_send("x_r", (0, 0), (0, 1), 0, left)
    for h in range(2):
        fs_send("c0", (0, 0), (1, 0), h, partner)

    @scoped("gather_rows")
    def gather_rows(name, h):
        arrive((name, h))
        if name == "x_2":
            fs_send("c2", (0, 2), (1, 2), h, partner, BLK // 4)
            return
        slot, onward, first = (3, right, 0) if name == "x_l" else (1, left, 1)
        if h == first:
            for q in (2 * h, 2 * h + 1):
                fs_send("x_2", (0, slot), (0, 2), q, onward, BLK // 4)
        fs_send(f"c{slot}", (0, slot), (1, slot), h, partner)

    def needs(w, ranks):
        for o in ranks:
            for origin in (o, (o[1], o[0])):
                if origin != (0, 0):
                    need(w, origin)

    @scoped("hidden_a")
    def hidden_a(dx):
        arrive(f"c{dx}")
        needs("u", ORDER[: KA // BLK])
        for n in range(HID // 256):
            cols = pl.ds(n * 256, 256)
            rows = fs[:, dx, :, 0:KA].reshape(2 * BLK, KA)
            hacc[min(dx, 2), :, cols] = dot(rows, up_all[0:KA, cols])

    @scoped("hidden")
    def hidden(dx):
        arrive(f"c{dx}")
        needs("u", ORDER)
        lo = 0 if dx == 2 else KA
        for n in range(HID // 256):
            cols = pl.ds(n * 256, 256)
            rows = fs[:, dx, :, lo:D].reshape(2 * BLK, D - lo)
            v = dot(rows, up_all[lo:D, cols])
            if lo:
                v = v + hacc[min(dx, 2), :, cols]
            v = jnp.maximum(v, 0.0)
            act[:, dx, :, cols] = (v * v).astype(BF16).reshape(2, BLK, 256)

    @scoped("product_a")
    def product_a(j):
        needs("d", ORDER[2 * j : 2 * j + 2])
        cols = pl.ds(j * CW, CW)
        psend[j] = dot(act[1].reshape(4 * BLK, HID), dn_all[:, cols]).astype(BF16).reshape(R, BLK, CW)
        send(("p", j), psend.at[j], prx.at[j], partner, "p", psend)

    @scoped("product_b")
    def product_b(j):
        cols = pl.ds(j * CW, CW)
        pown[j] = dot(act[0].reshape(4 * BLK, HID), dn_all[:, cols]).reshape(R, BLK, CW)

    LO, HI = pl.ds(0, HALF), pl.ds(HALF, HALF)

    def pair(j, dx, rows=slice(None)):
        return pown[j, dx, rows, :] + prx[j, dx, rows, :].astype(F32)

    @scoped("pair_sum")
    def pair_sum(j):
        arrive(("p", j))
        s2[j] = pair(j, 2).astype(BF16)
        send("mid", s2.at[j, LO, :], mid.at[j, LO, :], right, "s2", s2, ("mid", j), mid.at[j])
        send("mid", s2.at[j, HI, :], mid.at[j, HI, :], left, "s2", s2, ("mid", j), mid.at[j])
        s1[j, HI, :] = pair(j, 1, HI).astype(BF16)
        s3[j, LO, :] = pair(j, 3, LO).astype(BF16)
        send("fin", s1.at[j, HI, :], fin.at[j, 0, HI, :], right, "s1", s1, ("fin", j), fin.at[j])
        send("fin", s3.at[j, LO, :], fin.at[j, 1, LO, :], left, "s3", s3, ("fin", j), fin.at[j])
        macc[:, pl.ds(j * CW, CW)] = pair(j, 0)

    @scoped("middle")
    def middle(j):
        arrive(("mid", j))
        s1[j, LO, :] = (pair(j, 1, LO) + mid[j, LO, :].astype(F32)).astype(BF16)
        s3[j, HI, :] = (pair(j, 3, HI) + mid[j, HI, :].astype(F32)).astype(BF16)
        send("fin", s1.at[j, LO, :], fin.at[j, 0, LO, :], right, "s1", s1, ("fin", j), fin.at[j])
        send("fin", s3.at[j, HI, :], fin.at[j, 1, HI, :], left, "s3", s3, ("fin", j), fin.at[j])

    @scoped("total_sum")
    def total_sum(j):
        arrive(("fin", j))
        macc[:, pl.ds(j * CW, CW)] += fin[j, 0].astype(F32) + fin[j, 1].astype(F32)

    need("u", (0, 3))
    need("u", (0, 1))
    need("u", (2, 0))
    need("u", (3, 3))
    gather_rows("x_l", 0)
    gather_rows("x_r", 1)
    need("u", (1, 1))
    hidden_a(0)
    gather_rows("x_l", 1)
    gather_rows("x_r", 0)
    need("u", (2, 3))
    need("u", (2, 1))
    own_down(BP, BM)
    need("d", (3, 0))
    need("d", (1, 0))
    hidden_a(3)
    hidden_a(1)
    gather_rows("x_2", 0)
    gather_rows("x_2", 2)
    gather_rows("x_2", 1)
    gather_rows("x_2", 3)
    hidden(0)
    hidden(1)
    hidden(3)
    need("d", (2, 0))
    hidden(2)
    need("d", (0, 3))
    need("d", (0, 1))
    product_a(0)
    product_b(0)
    product_a(1)
    need("d", (3, 3))
    product_b(1)
    pair_sum(0)
    product_a(2)
    product_b(2)
    pair_sum(1)
    need("d", (1, 1))
    product_a(3)
    pair_sum(2)
    middle(0)
    product_b(3)
    middle(1)
    pair_sum(3)
    need("d", (2, 3))
    need("d", (2, 1))
    middle(2)
    product_a(4)
    total_sum(0)
    product_b(4)
    total_sum(1)
    middle(3)
    pair_sum(4)
    product_a(5)
    total_sum(2)
    product_b(5)
    product_a(6)
    total_sum(3)
    product_b(6)
    pair_sum(5)
    middle(4)
    product_a(7)
    pair_sum(6)
    product_b(7)
    pair_sum(7)
    middle(5)
    total_sum(4)
    middle(6)
    middle(7)
    total_sum(5)
    total_sum(6)
    total_sum(7)
    @scoped("last_norm")
    def last_norm(h):
        macc[half(h), :] += fs[0, 0, half(h), :].astype(F32)
        centre, factor = moments(macc[half(h), :])
        for r in range(16):
            c = cols_of(r)
            v = (macc[half(h), pl.ds(r * BLK, BLK)] - centre) * factor * g2[:, c]
            out[half(h), c] = v.astype(BF16)

    local["g2"].wait()
    for h in range(2):
        last_norm(h)

    @scoped("drain")
    def drain():
        for kind, key in ends:
            if kind == "s":
                wait(kind, key)

    drain()
    assert len(send_sems.index) == SENDS and len(recv_sems.index) == ARRIVALS


def far(v):
    return pltpu.with_memory_space_constraint(v, pltpu.HBM)


def per_device(q, kv, sink, doc, stream, ow, g1, up, dn, g2):
    vm, anyw = pl.BlockSpec(memory_space=pltpu.VMEM), pl.BlockSpec(memory_space=pl.ANY)
    smem = pl.BlockSpec(memory_space=pltpu.SMEM)
    return pl.pallas_call(
        kernel,
        out_shape=jax.ShapeDtypeStruct(stream.shape, BF16),
        in_specs=[anyw, anyw, smem, anyw, anyw, anyw, anyw, anyw, anyw, anyw],
        out_specs=vm,
        scratch_shapes=[
            pltpu.VMEM((1, D), F32),
            pltpu.VMEM((1, D), F32),
            pltpu.VMEM((1024, BLK), BF16),
            pltpu.VMEM((1024 + 2 * BLK, BLK), BF16),
            pltpu.VMEM((8, BLK), jnp.int32),
            pltpu.VMEM((16, BLK), jnp.int32),
            pltpu.VMEM((24, BLK), F32),
            pltpu.VMEM((BLK, D), BF16),
            pltpu.VMEM((1024, D), BF16),
            pltpu.VMEM((1024, BLK), BF16),
            pltpu.VMEM((BLK, 1024), BF16),
            pltpu.VMEM((BLK, D), F32),
            pltpu.VMEM((D, HID), BF16),
            pltpu.VMEM((HID, D), BF16),
            pltpu.VMEM((2, R, BLK, D), BF16),
            pltpu.VMEM((3, 2 * BLK, HID), F32),
            pltpu.VMEM((2, R, BLK, HID), BF16),
            pltpu.VMEM((NCH, R, BLK, CW), BF16),
            pltpu.VMEM((NCH, R, BLK, CW), BF16),
            pltpu.VMEM((NCH, R, BLK, CW), F32),
            pltpu.VMEM((NCH, BLK, CW), BF16),
            pltpu.VMEM((NCH, BLK, CW), BF16),
            pltpu.VMEM((NCH, BLK, CW), BF16),
            pltpu.VMEM((NCH, BLK, CW), BF16),
            pltpu.VMEM((NCH, 2, BLK, CW), BF16),
            pltpu.VMEM((BLK, D), F32),
            pltpu.SemaphoreType.DMA((SENDS,)),
            pltpu.SemaphoreType.DMA((ARRIVALS,)),
            pltpu.SemaphoreType.DMA((9,)),
        ],
        compiler_params=pltpu.CompilerParams(
            collective_id=0, has_side_effects=True, vmem_limit_bytes=48 * 1024 * 1024
        ),
        name="layer",
    )(
        far(q), far(kv.reshape(1024, BLK)), far(sink), far(doc.reshape(8, BLK)), far(stream), far(ow),
        far(g1.reshape(1, D)), far(up), far(dn), far(g2.reshape(1, D)),
    )


def solution(mesh):
    placed = (
        P("sp", "tp"),
        P("sp", "tp", None),
        P("tp"),
        P("sp"),
        P(("sp", "tp"), None),
        P(),
        P(),
        P("sp", "tp"),
        P("tp", "sp"),
        P(),
    )
    return jax.shard_map(
        per_device, mesh=mesh, in_specs=placed, out_specs=P(("sp", "tp"), None), check_vma=False
    )
```

```python
import functools

import jax
import jax.numpy as jnp
from jax import lax
from jax.experimental import pallas as pl
from jax.experimental.pallas import tpu as pltpu
from jax.sharding import PartitionSpec as P

MESH = pl.DeviceIdType.MESH
F32 = jnp.float32
BF16 = jnp.bfloat16
NEG_LARGE = -1e30
NORM_EPS = 1e-05
R = 4
BLK = 128
D = 2048
HID = 1024
NCH = 8
CW = D // NCH
SENDS, ARRIVALS = 13, 65

ORDER = [
    (0, 0), (1, 0), (3, 0), (0, 1), (0, 3), (3, 3), (3, 1), (1, 1),
    (1, 3), (2, 0), (0, 2), (3, 2), (2, 3), (2, 1), (1, 2), (2, 2),
]
RANK = {o: i for i, o in enumerate(ORDER)}

AP, AM, BP, BM = (1, 0), (-1, 0), (0, 1), (0, -1)
ONWARD = {
    (3, 0): [(AP, 0), (BP, None), (BM, None)],
    (1, 0): [(AM, 1), (BP, None), (BM, None)],
    (2, 0): [(BP, None), (BM, None)],
    (0, 3): [(BP, 0)],
    (0, 1): [(BM, 1)],
    (3, 3): [(BP, None)],
    (1, 1): [(BM, None)],
    (2, 3): [(BP, 0)],
    (2, 1): [(BM, 1)],
}
TOGETHER = (((3, 1), (1, 3)), ((0, 2), (3, 2), (1, 2), (2, 2)))
KA = HID


def nt_dot(a, b):
    return lax.dot_general(a, b, (((1,), (1,)), ((), ())), preferred_element_type=F32)


def dot(a, b):
    return jnp.dot(a, b, preferred_element_type=F32)


def moments(x):
    centre = jnp.mean(x, axis=-1, keepdims=True)
    shifted = x - centre
    return centre, lax.rsqrt(jnp.mean(shifted * shifted, axis=-1, keepdims=True) + NORM_EPS)


def scoped(name):
    def wrap(f):
        @functools.wraps(f)
        def run(*args):
            tag = "_".join("".join(c for c in str(v) if c.isalnum()) for v in args if isinstance(v, (int, str, tuple)))
            with jax.named_scope(f"{name}#v={tag}"):
                return f(*args)

        return run

    return wrap


class Sems:
    def __init__(self):
        self.index = {}

    def at(self, key):
        return self.index.setdefault(key, len(self.index))


def kernel(
    q_h, kv_h, sink_s, doc_h, st_h, ow_h, g1_h, up_h, dn_h, g2_h, out,
    g1, g2, qv, kvx, docv, doc_lr, docx, stv, owv, att_own, att_all, xbuf,
    up_all, dn_all, fs, hacc, act, psend, prx, pown, s1, s2, s3, mid, fin, macc,
    ss, rs, ls,
):
    sp, tp = lax.axis_index("sp"), lax.axis_index("tp")
    z, y = sp // R, sp % R
    x, core = tp // 2, tp % 2
    stride_a, stride_b = 1 + 3 * core, 4 - 3 * core
    a = y * (1 - core) + z * core
    b = z * (1 - core) + y * core

    def sp_of(da, db):
        return ((a + da) % R) * stride_a + ((b + db) % R) * stride_b

    partner = (sp, x * 2 + (1 - core))
    right = (sp, ((x + 1) % R) * 2 + core)
    left = (sp, ((x + R - 1) % R) * 2 + core)
    sp_next, sp_prev = (sp + 1) % 16, (sp + 15) % 16

    barrier = pltpu.get_barrier_semaphore()
    greet = [(sp, (tp + i) % 8) for i in range(1, 8)]
    greet += [(sp_of(da, db), tp) for da, db in ((1, 0), (3, 0), (0, 1), (0, 3))]
    greet += [(sp_next, tp), (sp_prev, tp)]
    for dev in greet:
        pl.semaphore_signal(barrier, inc=1, device_id=dev, device_id_type=MESH)
    local_names = ["kv", "doc", "up", "q", "st", "ow", "dn", "g1", "g2"]
    pairs = {
        "kv": (kv_h, kvx.at[pl.ds(BLK, 1024), :]),
        "doc": (doc_h, docv),
        "q": (q_h, qv),
        "up": (up_h, up_all.at[pl.ds(0, BLK), :]),
        "dn": (dn_h, dn_all.at[:, pl.ds(0, BLK)]),
        "st": (st_h, stv),
        "ow": (ow_h, owv),
        "g1": (g1_h, g1),
        "g2": (g2_h, g2),
    }
    local = {n: pltpu.make_async_copy(*pairs[n], ls.at[i]) for i, n in enumerate(local_names)}
    for n in local_names:
        local[n].start()

    pl.semaphore_wait(barrier, len(greet))

    send_sems, recv_sems = Sems(), Sems()
    ends = {}
    waited = set()

    def send(key, src, dst, dev, group, whole, with_key=None, with_dst=None):
        pltpu.make_async_remote_copy(
            src_ref=src, dst_ref=dst, send_sem=ss.at[send_sems.at(group)],
            recv_sem=rs.at[recv_sems.at(with_key or key)], device_id=dev, device_id_type=MESH,
        ).start()
        ends[("s", group)] = whole
        ends[("r", with_key or key)] = dst if with_dst is None else with_dst

    def wait(kind, key):
        ref = ends[(kind, key)]
        i = (send_sems if kind == "s" else recv_sems).at(key)
        copy = pltpu.make_async_remote_copy(
            src_ref=ref, dst_ref=ref, send_sem=ss.at[i], recv_sem=rs.at[i], device_id=partner, device_id_type=MESH
        )
        copy.wait_send() if kind == "s" else copy.wait_recv()

    def arrive(key):
        if key not in waited:
            waited.add(key)
            wait("r", key)

    local["kv"].wait()
    local["doc"].wait()
    rim = kvx.at[pl.ds(0, 2 * BLK), :]
    for src, dst, dev in ((1024, 0, sp_next), (BLK, 1024 + BLK, sp_prev)):
        rows = kvx.at[pl.ds(src, BLK), :], kvx.at[pl.ds(dst, BLK), :]
        send("kv", *rows, (dev, tp), "kv", rim, "kv", rim)
    send("doc", docv, doc_lr.at[pl.ds(0, 8), :], (sp_next, tp), "doc", doc_lr, "doc", doc_lr)
    send("doc", docv, doc_lr.at[pl.ds(8, 8), :], (sp_prev, tp), "doc", doc_lr, "doc", doc_lr)

    def block(w, origin, at, half):
        ra, rb = (origin[0] - at[0]) % R, (origin[1] - at[1]) % R
        r0, r1 = RANK[(ra, rb)], RANK[(rb, ra)]
        slot = (r0 + core * (r1 - r0)) * BLK
        size = BLK if w == "u" else HID
        lo, n = {None: (0, size), 0: (0, size // 2), 1: (size // 2, size // 2)}[half]
        if w == "u":
            return up_all.at[pl.ds(pl.multiple_of(slot + lo, BLK // 2), n), :]
        return dn_all.at[pl.ds(lo, n), pl.ds(pl.multiple_of(slot, BLK), BLK)]

    def pass_on(w, origin, to, half=None):
        rel = ((origin[0] - to[0]) % R, (origin[1] - to[1]) % R)
        held = up_all if w == "u" else dn_all
        together = {o: g for g in TOGETHER for o in g}.get(rel, (rel,)) if w == "u" else (rel,)
        n = len(together) * BLK
        send(
            (w, rel), block(w, origin, (0, 0), half), block(w, origin, to, half),
            (sp_of(to[0] % R, to[1] % R), tp),
            w, held.at[pl.ds(0, 15 * BLK), :] if w == "u" else held.at[:, pl.ds(0, 15 * BLK)],
            (w, together), held.at[pl.ds(0, n), :] if w == "u" else held.at[:, pl.ds(0, n)],
        )

    relayed = set()

    @scoped("need")
    def need(w, origin):
        if (w, origin) in relayed:
            return
        relayed.add((w, origin))
        arrive((w, {o: g for g in TOGETHER for o in g}.get(origin, (origin,)) if w == "u" else (origin,)))
        for to, h in ONWARD.get(origin, ()):
            pass_on(w, origin, to, h)

    def own_down(*ways):
        for to in ways:
            pass_on("d", (0, 0), to)

    local["up"].wait()
    for to in (AP, AM):
        pass_on("u", (0, 0), to)
    local["dn"].wait()
    own_down(AP, AM)

    local["q"].wait()
    docx[pl.ds(8, 8), :] = docv[...].astype(F32)
    row = lax.broadcasted_iota(jnp.int32, (BLK, BLK), 0)
    col = lax.broadcasted_iota(jnp.int32, (BLK, BLK), 1)
    low = col < 64
    a2a_send, a2a_recv = send_sems.at("a2a"), recv_sems.at("a2a")
    ends[("s", "a2a")] = ends[("r", "a2a")] = att_own.at[pl.ds(0, 7 * BLK), :]

    def attended(blk):
        rows = pl.ds(pl.multiple_of(blk * BLK, BLK), BLK)
        qf = qv[rows, :].astype(F32) * 0.125
        q2 = jnp.concatenate(
            [jnp.where(low, qf, 0.0), jnp.where(low, pltpu.roll(qf, 64, 1), 0.0)], axis=0
        ).astype(BF16)
        kvb = kvx[pl.ds(pl.multiple_of(blk * BLK, BLK), 3 * BLK), :]
        s = nt_dot(q2, kvb)
        dq = jnp.broadcast_to(docx[pl.ds(blk + 8, 1), :], (BLK, BLK)).T
        same = [jnp.broadcast_to(docx[pl.ds(blk + 7 + j, 1), :], (BLK, BLK)) == dq for j in range(3)]
        same[0] = same[0] & (col >= row)
        same[2] = same[2] & (col <= row)
        weights, scale = [], []
        for h in range(2):
            sink = sink_s[h]
            t = [
                jnp.where(same[j], s[h * BLK : (h + 1) * BLK, j * BLK : (j + 1) * BLK], NEG_LARGE)
                for j in range(3)
            ]
            top = jnp.max(jnp.maximum(jnp.maximum(t[0], t[1]), t[2]), axis=-1, keepdims=True)
            top = jnp.maximum(top, sink)
            p = [jnp.exp(v - top) for v in t]
            total = jnp.sum(p[0] + p[1] + p[2], axis=-1, keepdims=True) + jnp.exp(sink - top)
            weights.append(jnp.concatenate(p, axis=1).astype(BF16))
            scale.append(1.0 / total)
        o = dot(jnp.concatenate(weights, axis=0), kvb)
        o0, o1 = o[:BLK] * scale[0], o[BLK:] * scale[1]
        return jnp.where(low, pltpu.roll(o0, 64, 1), o1).astype(BF16)

    def hand_out(blk):
        rows = pl.ds(pl.multiple_of(blk * BLK, BLK), BLK)
        mine = pl.ds(pl.multiple_of(tp * BLK, BLK), BLK)

        @pl.when(blk != tp)
        def _():
            pltpu.make_async_remote_copy(
                src_ref=att_own.at[rows, :], dst_ref=att_all.at[:, mine],
                send_sem=ss.at[a2a_send], recv_sem=rs.at[a2a_recv],
                device_id=(sp, blk), device_id_type=MESH,
            ).start()

        @pl.when(blk == tp)
        def _():
            att_all[:, mine] = att_own[rows, :]

    @scoped("attend")
    def attend(first, second):
        values = [attended(first), attended(second)]
        for blk, v in zip((first, second), values):
            att_own[pl.ds(pl.multiple_of(blk * BLK, BLK), BLK), :] = v
        for blk in (first, second):
            hand_out(blk)

    def inner(i, carry):
        attend(2 * i + 1, 2 * i + 2)
        return carry

    lax.fori_loop(0, 2, inner, 0)
    for to in (BP, BM):
        pass_on("u", (0, 0), to)
    lax.fori_loop(2, 3, inner, 0)
    arrive("kv")
    arrive("doc")
    docx[pl.ds(0, 8), :] = jnp.where(sp == 0, -1.0, doc_lr[pl.ds(0, 8), :].astype(F32))
    docx[pl.ds(16, 8), :] = jnp.where(sp == 15, -1.0, doc_lr[pl.ds(8, 8), :].astype(F32))

    def outer(i, carry):
        attend(i, i + 7)
        return carry

    lax.fori_loop(0, 1, outer, 0)

    @scoped("a2a_wait")
    def a2a_wait():
        local["ow"].wait()
        local["st"].wait()
        local["g1"].wait()
        arrive("a2a")

    a2a_wait()
    need("u", (3, 0))
    need("u", (1, 0))

    def project(n):
        cols = pl.ds(n * 512, 512)
        xbuf[:, cols] = dot(att_all[...], owv[:, cols]) + stv[:, cols].astype(F32)

    @scoped("projection")
    def projection():
        for n in range(4):
            project(n)

    projection()

    def cols_of(rank):
        dy, dz = ORDER[rank]
        return pl.ds(pl.multiple_of((((z + dz) % R) * R + (y + dy) % R) * BLK, BLK), BLK)

    HALF = BLK // 2
    half = lambda h: pl.ds(h * HALF, HALF)

    def fs_send(name, src, dst, i, dev, n=HALF):
        rows = pl.ds(i * n, n)
        to_partner = name[0] == "c"
        send(
            (name, i), fs.at[src[0], src[1], rows, :], fs.at[dst[0], dst[1], rows, :], dev,
            "c" if to_partner else name, fs.at[0] if to_partner else fs.at[0, 0],
            name if to_partner else None, fs.at[1, dst[1]] if to_partner else None,
        )

    @scoped("first_norm")
    def first_norm(h):
        centre, factor = moments(xbuf[half(h), :])
        for r in range(16):
            c = cols_of(r)
            v = (xbuf[half(h), c] - centre) * factor * g1[:, c]
            fs[0, 0, half(h), pl.ds(r * BLK, BLK)] = v.astype(BF16)

    for h in range(2):
        first_norm(h)
        if h == 0:
            fs_send("x_l", (0, 0), (0, 3), 0, right)
    fs_send("x_r", (0, 0), (0, 1), 1, left)
    fs_send("x_l", (0, 0), (0, 3), 1, right)
    fs_send("x_r", (0, 0), (0, 1), 0, left)
    for h in range(2):
        fs_send("c0", (0, 0), (1, 0), h, partner)

    @scoped("gather_rows")
    def gather_rows(name, h):
        arrive((name, h))
        if name == "x_2":
            fs_send("c2", (0, 2), (1, 2), h, partner, BLK // 4)
            return
        slot, onward, first = (3, right, 0) if name == "x_l" else (1, left, 1)
        if h == first:
            for q in (2 * h, 2 * h + 1):
                fs_send("x_2", (0, slot), (0, 2), q, onward, BLK // 4)
        fs_send(f"c{slot}", (0, slot), (1, slot), h, partner)

    def needs(w, ranks):
        for o in ranks:
            for origin in (o, (o[1], o[0])):
                if origin != (0, 0):
                    need(w, origin)

    @scoped("hidden_a")
    def hidden_a(dx):
        arrive(f"c{dx}")
        needs("u", ORDER[: KA // BLK])
        for n in range(HID // 256):
            cols = pl.ds(n * 256, 256)
            rows = fs[:, dx, :, 0:KA].reshape(2 * BLK, KA)
            hacc[min(dx, 2), :, cols] = dot(rows, up_all[0:KA, cols])

    @scoped("hidden")
    def hidden(dx):
        arrive(f"c{dx}")
        needs("u", ORDER)
        lo = 0 if dx == 2 else KA
        for n in range(HID // 256):
            cols = pl.ds(n * 256, 256)
            rows = fs[:, dx, :, lo:D].reshape(2 * BLK, D - lo)
            v = dot(rows, up_all[lo:D, cols])
            if lo:
                v = v + hacc[min(dx, 2), :, cols]
            v = jnp.maximum(v, 0.0)
            act[:, dx, :, cols] = (v * v).astype(BF16).reshape(2, BLK, 256)

    @scoped("product_a")
    def product_a(j):
        needs("d", ORDER[2 * j : 2 * j + 2])
        cols = pl.ds(j * CW, CW)
        for two in (pl.ds(0, 2), pl.ds(2, 2)):
            v = dot(act[1, two].reshape(2 * BLK, HID), dn_all[:, cols])
            psend[j, two] = v.astype(BF16).reshape(2, BLK, CW)
        send(("p", j), psend.at[j], prx.at[j], partner, "p", psend)

    @scoped("product_b")
    def product_b(j):
        cols = pl.ds(j * CW, CW)
        for two in (pl.ds(0, 2), pl.ds(2, 2)):
            pown[j, two] = dot(act[0, two].reshape(2 * BLK, HID), dn_all[:, cols]).reshape(2, BLK, CW)

    LO, HI = pl.ds(0, HALF), pl.ds(HALF, HALF)

    def pair(j, dx, rows=slice(None)):
        return pown[j, dx, rows, :] + prx[j, dx, rows, :].astype(F32)

    @scoped("pair_sum")
    def pair_sum(j):
        arrive(("p", j))
        s2[j] = pair(j, 2).astype(BF16)
        send("mid", s2.at[j, LO, :], mid.at[j, LO, :], right, "s2", s2, ("mid", j), mid.at[j])
        send("mid", s2.at[j, HI, :], mid.at[j, HI, :], left, "s2", s2, ("mid", j), mid.at[j])
        if j < 6:
            direct(j)
        macc[:, pl.ds(j * CW, CW)] = pair(j, 0)

    @scoped("direct")
    def direct(j):
        s1[j, HI, :] = pair(j, 1, HI).astype(BF16)
        s3[j, LO, :] = pair(j, 3, LO).astype(BF16)
        send("fin", s1.at[j, HI, :], fin.at[j, 0, HI, :], right, "s1", s1, ("fin", j), fin.at[j])
        send("fin", s3.at[j, LO, :], fin.at[j, 1, LO, :], left, "s3", s3, ("fin", j), fin.at[j])

    @scoped("middle")
    def middle(j):
        arrive(("mid", j))
        s1[j, LO, :] = (pair(j, 1, LO) + mid[j, LO, :].astype(F32)).astype(BF16)
        s3[j, HI, :] = (pair(j, 3, HI) + mid[j, HI, :].astype(F32)).astype(BF16)
        send("fin", s1.at[j, LO, :], fin.at[j, 0, LO, :], right, "s1", s1, ("fin", j), fin.at[j])
        send("fin", s3.at[j, HI, :], fin.at[j, 1, HI, :], left, "s3", s3, ("fin", j), fin.at[j])

    @scoped("total_sum")
    def total_sum(j):
        arrive(("fin", j))
        macc[:, pl.ds(j * CW, CW)] += fin[j, 0].astype(F32) + fin[j, 1].astype(F32)

    need("u", (0, 3))
    need("u", (0, 1))
    need("u", (2, 0))
    need("u", (3, 3))
    gather_rows("x_l", 0)
    gather_rows("x_r", 1)
    need("u", (1, 1))
    hidden_a(0)
    gather_rows("x_l", 1)
    gather_rows("x_r", 0)
    need("u", (2, 3))
    need("u", (2, 1))
    own_down(BP, BM)
    need("d", (3, 0))
    need("d", (1, 0))
    hidden_a(3)
    hidden_a(1)
    gather_rows("x_2", 0)
    gather_rows("x_2", 2)
    gather_rows("x_2", 1)
    gather_rows("x_2", 3)
    hidden(0)
    hidden(1)
    hidden(3)
    need("d", (0, 3))
    need("d", (0, 1))
    need("d", (2, 0))
    hidden(2)
    product_a(0)
    product_b(0)
    product_a(1)
    need("d", (3, 3))
    pair_sum(0)
    product_b(1)
    product_a(2)
    pair_sum(1)
    product_b(2)
    need("d", (1, 1))
    pair_sum(2)
    product_a(3)
    middle(0)
    product_b(3)
    middle(1)
    product_a(4)
    pair_sum(3)
    product_b(4)
    middle(2)
    pair_sum(4)
    need("d", (2, 3))
    need("d", (2, 1))
    middle(3)
    product_a(5)
    product_b(5)
    product_a(6)
    pair_sum(5)
    product_b(6)
    middle(4)
    product_a(7)
    pair_sum(6)
    product_b(7)
    pair_sum(7)
    middle(5)
    direct(6)
    direct(7)
    middle(6)
    total_sum(0)
    total_sum(1)
    total_sum(2)
    total_sum(3)
    total_sum(4)
    middle(7)
    total_sum(5)
    total_sum(6)
    total_sum(7)
    @scoped("last_norm")
    def last_norm(h):
        macc[half(h), :] += fs[0, 0, half(h), :].astype(F32)
        centre, factor = moments(macc[half(h), :])
        for r in range(16):
            c = cols_of(r)
            v = (macc[half(h), pl.ds(r * BLK, BLK)] - centre) * factor * g2[:, c]
            out[half(h), c] = v.astype(BF16)

    local["g2"].wait()
    for h in range(2):
        last_norm(h)

    @scoped("drain")
    def drain():
        for kind, key in ends:
            if kind == "s":
                wait(kind, key)

    drain()
    assert len(send_sems.index) == SENDS and len(recv_sems.index) == ARRIVALS


def far(v):
    return pltpu.with_memory_space_constraint(v, pltpu.HBM)


def per_device(q, kv, sink, doc, stream, ow, g1, up, dn, g2):
    vm, anyw = pl.BlockSpec(memory_space=pltpu.VMEM), pl.BlockSpec(memory_space=pl.ANY)
    smem = pl.BlockSpec(memory_space=pltpu.SMEM)
    return pl.pallas_call(
        kernel,
        out_shape=jax.ShapeDtypeStruct(stream.shape, BF16),
        in_specs=[anyw, anyw, smem, anyw, anyw, anyw, anyw, anyw, anyw, anyw],
        out_specs=vm,
        scratch_shapes=[
            pltpu.VMEM((1, D), F32),
            pltpu.VMEM((1, D), F32),
            pltpu.VMEM((1024, BLK), BF16),
            pltpu.VMEM((1024 + 2 * BLK, BLK), BF16),
            pltpu.VMEM((8, BLK), jnp.int32),
            pltpu.VMEM((16, BLK), jnp.int32),
            pltpu.VMEM((24, BLK), F32),
            pltpu.VMEM((BLK, D), BF16),
            pltpu.VMEM((1024, D), BF16),
            pltpu.VMEM((1024, BLK), BF16),
            pltpu.VMEM((BLK, 1024), BF16),
            pltpu.VMEM((BLK, D), F32),
            pltpu.VMEM((D, HID), BF16),
            pltpu.VMEM((HID, D), BF16),
            pltpu.VMEM((2, R, BLK, D), BF16),
            pltpu.VMEM((3, 2 * BLK, HID), F32),
            pltpu.VMEM((2, R, BLK, HID), BF16),
            pltpu.VMEM((NCH, R, BLK, CW), BF16),
            pltpu.VMEM((NCH, R, BLK, CW), BF16),
            pltpu.VMEM((NCH, R, BLK, CW), F32),
            pltpu.VMEM((NCH, BLK, CW), BF16),
            pltpu.VMEM((NCH, BLK, CW), BF16),
            pltpu.VMEM((NCH, BLK, CW), BF16),
            pltpu.VMEM((NCH, BLK, CW), BF16),
            pltpu.VMEM((NCH, 2, BLK, CW), BF16),
            pltpu.VMEM((BLK, D), F32),
            pltpu.SemaphoreType.DMA((SENDS,)),
            pltpu.SemaphoreType.DMA((ARRIVALS,)),
            pltpu.SemaphoreType.DMA((9,)),
        ],
        compiler_params=pltpu.CompilerParams(
            collective_id=0, has_side_effects=True, vmem_limit_bytes=48 * 1024 * 1024
        ),
        name="layer",
    )(
        far(q), far(kv.reshape(1024, BLK)), far(sink), far(doc.reshape(8, BLK)), far(stream), far(ow),
        far(g1.reshape(1, D)), far(up), far(dn), far(g2.reshape(1, D)),
    )


def solution(mesh):
    placed = (
        P("sp", "tp"),
        P("sp", "tp", None),
        P("tp"),
        P("sp"),
        P(("sp", "tp"), None),
        P(),
        P(),
        P("sp", "tp"),
        P("tp", "sp"),
        P(),
    )
    return jax.shard_map(
        per_device, mesh=mesh, in_specs=placed, out_specs=P(("sp", "tp"), None), check_vma=False
    )
```

```python
import functools

import jax
import jax.numpy as jnp
from jax import lax
from jax.experimental import pallas as pl
from jax.experimental.pallas import tpu as pltpu
from jax.sharding import PartitionSpec as P

MESH = pl.DeviceIdType.MESH
F32 = jnp.float32
BF16 = jnp.bfloat16
NEG_LARGE = -1e30
NORM_EPS = 1e-05
R = 4
BLK = 128
D = 2048
HID = 1024
NCH = 8
CW = D // NCH
SENDS, ARRIVALS = 13, 66

ORDER = [
    (0, 0), (1, 0), (3, 0), (0, 1), (0, 3), (3, 3), (3, 1), (1, 1),
    (1, 3), (2, 0), (0, 2), (3, 2), (2, 3), (2, 1), (1, 2), (2, 2),
]
RANK = {o: i for i, o in enumerate(ORDER)}

AP, AM, BP, BM = (1, 0), (-1, 0), (0, 1), (0, -1)
ONWARD = {
    (3, 0): [(AP, 0), (BP, None), (BM, None)],
    (1, 0): [(AM, 1), (BP, None), (BM, None)],
    (2, 0): [(BP, None), (BM, None)],
}
ONWARD |= {(da, 3): [(BP, 0)] for da in range(R)} | {(da, 1): [(BM, 1)] for da in range(R)}
TOGETHER = (((0, 2), (3, 2), (1, 2), (2, 2)),)
KA = HID


def nt_dot(a, b):
    return lax.dot_general(a, b, (((1,), (1,)), ((), ())), preferred_element_type=F32)


def dot(a, b):
    return jnp.dot(a, b, preferred_element_type=F32)


def moments(x):
    centre = jnp.mean(x, axis=-1, keepdims=True)
    shifted = x - centre
    return centre, lax.rsqrt(jnp.mean(shifted * shifted, axis=-1, keepdims=True) + NORM_EPS)


def scoped(name):
    def wrap(f):
        @functools.wraps(f)
        def run(*args):
            tag = "_".join("".join(c for c in str(v) if c.isalnum()) for v in args if isinstance(v, (int, str, tuple)))
            with jax.named_scope(f"{name}#v={tag}"):
                return f(*args)

        return run

    return wrap


class Sems:
    def __init__(self):
        self.index = {}

    def at(self, key):
        return self.index.setdefault(key, len(self.index))


def kernel(
    q_h, kv_h, sink_s, doc_h, st_h, ow_h, g1_h, up_h, dn_h, g2_h, out,
    g1, g2, qv, kvx, docv, doc_lr, docx, stv, owv, att_own, att_all, xbuf,
    up_all, dn_all, fs, hacc, act, psend, prx, pown, s1, s2, s3, mid, fin, macc,
    ss, rs, ls,
):
    sp, tp = lax.axis_index("sp"), lax.axis_index("tp")
    z, y = sp // R, sp % R
    x, core = tp // 2, tp % 2
    stride_a, stride_b = 1 + 3 * core, 4 - 3 * core
    a = y * (1 - core) + z * core
    b = z * (1 - core) + y * core

    def sp_of(da, db):
        return ((a + da) % R) * stride_a + ((b + db) % R) * stride_b

    partner = (sp, x * 2 + (1 - core))
    right = (sp, ((x + 1) % R) * 2 + core)
    left = (sp, ((x + R - 1) % R) * 2 + core)
    sp_next, sp_prev = (sp + 1) % 16, (sp + 15) % 16

    barrier = pltpu.get_barrier_semaphore()
    greet = [(sp, (tp + i) % 8) for i in range(1, 8)]
    greet += [(sp_of(da, db), tp) for da, db in ((1, 0), (3, 0), (0, 1), (0, 3))]
    greet += [(sp_next, tp), (sp_prev, tp)]
    for dev in greet:
        pl.semaphore_signal(barrier, inc=1, device_id=dev, device_id_type=MESH)
    local_names = ["kv", "doc", "up", "q", "st", "ow", "dn", "g1", "g2"]
    pairs = {
        "kv": (kv_h, kvx.at[pl.ds(BLK, 1024), :]),
        "doc": (doc_h, docv),
        "q": (q_h, qv),
        "up": (up_h, up_all.at[pl.ds(0, BLK), :]),
        "dn": (dn_h, dn_all.at[:, pl.ds(0, BLK)]),
        "st": (st_h, stv),
        "ow": (ow_h, owv),
        "g1": (g1_h, g1),
        "g2": (g2_h, g2),
    }
    local = {n: pltpu.make_async_copy(*pairs[n], ls.at[i]) for i, n in enumerate(local_names)}
    for n in local_names:
        local[n].start()

    pl.semaphore_wait(barrier, len(greet))

    send_sems, recv_sems = Sems(), Sems()
    ends = {}
    waited = set()

    def send(key, src, dst, dev, group, whole, with_key=None, with_dst=None):
        pltpu.make_async_remote_copy(
            src_ref=src, dst_ref=dst, send_sem=ss.at[send_sems.at(group)],
            recv_sem=rs.at[recv_sems.at(with_key or key)], device_id=dev, device_id_type=MESH,
        ).start()
        ends[("s", group)] = whole
        ends[("r", with_key or key)] = dst if with_dst is None else with_dst

    def wait(kind, key):
        ref = ends[(kind, key)]
        i = (send_sems if kind == "s" else recv_sems).at(key)
        copy = pltpu.make_async_remote_copy(
            src_ref=ref, dst_ref=ref, send_sem=ss.at[i], recv_sem=rs.at[i], device_id=partner, device_id_type=MESH
        )
        copy.wait_send() if kind == "s" else copy.wait_recv()

    def arrive(key):
        if key not in waited:
            waited.add(key)
            wait("r", key)

    local["kv"].wait()
    local["doc"].wait()
    rim = kvx.at[pl.ds(0, 2 * BLK), :]
    for src, dst, dev in ((1024, 0, sp_next), (BLK, 1024 + BLK, sp_prev)):
        rows = kvx.at[pl.ds(src, BLK), :], kvx.at[pl.ds(dst, BLK), :]
        send("kv", *rows, (dev, tp), "kv", rim, "kv", rim)
    send("doc", docv, doc_lr.at[pl.ds(0, 8), :], (sp_next, tp), "doc", doc_lr, "doc", doc_lr)
    send("doc", docv, doc_lr.at[pl.ds(8, 8), :], (sp_prev, tp), "doc", doc_lr, "doc", doc_lr)

    def block(w, origin, at, half):
        ra, rb = (origin[0] - at[0]) % R, (origin[1] - at[1]) % R
        r0, r1 = RANK[(ra, rb)], RANK[(rb, ra)]
        slot = (r0 + core * (r1 - r0)) * BLK
        size = BLK if w == "u" else HID
        lo, n = {None: (0, size), 0: (0, size // 2), 1: (size // 2, size // 2)}[half]
        if w == "u":
            return up_all.at[pl.ds(pl.multiple_of(slot + lo, BLK // 2), n), :]
        return dn_all.at[pl.ds(lo, n), pl.ds(pl.multiple_of(slot, BLK), BLK)]

    def pass_on(w, origin, to, half=None):
        rel = ((origin[0] - to[0]) % R, (origin[1] - to[1]) % R)
        held = up_all if w == "u" else dn_all
        together = {o: g for g in TOGETHER for o in g}.get(rel, (rel,)) if w == "u" else (rel,)
        n = len(together) * BLK
        send(
            (w, rel), block(w, origin, (0, 0), half), block(w, origin, to, half),
            (sp_of(to[0] % R, to[1] % R), tp),
            w, held.at[pl.ds(0, 15 * BLK), :] if w == "u" else held.at[:, pl.ds(0, 15 * BLK)],
            (w, together), held.at[pl.ds(0, n), :] if w == "u" else held.at[:, pl.ds(0, n)],
        )

    relayed = set()

    @scoped("need")
    def need(w, origin):
        if (w, origin) in relayed:
            return
        relayed.add((w, origin))
        arrive((w, {o: g for g in TOGETHER for o in g}.get(origin, (origin,)) if w == "u" else (origin,)))
        for to, h in ONWARD.get(origin, ()):
            pass_on(w, origin, to, h)

    def own_down(*ways):
        for to in ways:
            pass_on("d", (0, 0), to)

    local["up"].wait()
    for to in (AP, AM):
        pass_on("u", (0, 0), to)
    local["dn"].wait()
    own_down(AP, AM)

    local["q"].wait()
    docx[pl.ds(8, 8), :] = docv[...].astype(F32)
    row = lax.broadcasted_iota(jnp.int32, (BLK, BLK), 0)
    col = lax.broadcasted_iota(jnp.int32, (BLK, BLK), 1)
    low = col < 64
    a2a_send, a2a_recv = send_sems.at("a2a"), recv_sems.at("a2a")
    ends[("s", "a2a")] = ends[("r", "a2a")] = att_own.at[pl.ds(0, 7 * BLK), :]

    def attended(blk):
        rows = pl.ds(pl.multiple_of(blk * BLK, BLK), BLK)
        qf = qv[rows, :].astype(F32) * 0.125
        q2 = jnp.concatenate(
            [jnp.where(low, qf, 0.0), jnp.where(low, pltpu.roll(qf, 64, 1), 0.0)], axis=0
        ).astype(BF16)
        kvb = kvx[pl.ds(pl.multiple_of(blk * BLK, BLK), 3 * BLK), :]
        s = nt_dot(q2, kvb)
        dq = jnp.broadcast_to(docx[pl.ds(blk + 8, 1), :], (BLK, BLK)).T
        same = [jnp.broadcast_to(docx[pl.ds(blk + 7 + j, 1), :], (BLK, BLK)) == dq for j in range(3)]
        same[0] = same[0] & (col >= row)
        same[2] = same[2] & (col <= row)
        weights, scale = [], []
        for h in range(2):
            sink = sink_s[h]
            t = [
                jnp.where(same[j], s[h * BLK : (h + 1) * BLK, j * BLK : (j + 1) * BLK], NEG_LARGE)
                for j in range(3)
            ]
            top = jnp.max(jnp.maximum(jnp.maximum(t[0], t[1]), t[2]), axis=-1, keepdims=True)
            top = jnp.maximum(top, sink)
            p = [jnp.exp(v - top) for v in t]
            total = jnp.sum(p[0] + p[1] + p[2], axis=-1, keepdims=True) + jnp.exp(sink - top)
            weights.append(jnp.concatenate(p, axis=1).astype(BF16))
            scale.append(1.0 / total)
        o = dot(jnp.concatenate(weights, axis=0), kvb)
        o0, o1 = o[:BLK] * scale[0], o[BLK:] * scale[1]
        return jnp.where(low, pltpu.roll(o0, 64, 1), o1).astype(BF16)

    def hand_out(blk):
        rows = pl.ds(pl.multiple_of(blk * BLK, BLK), BLK)
        mine = pl.ds(pl.multiple_of(tp * BLK, BLK), BLK)

        @pl.when(blk != tp)
        def _():
            pltpu.make_async_remote_copy(
                src_ref=att_own.at[rows, :], dst_ref=att_all.at[:, mine],
                send_sem=ss.at[a2a_send], recv_sem=rs.at[a2a_recv],
                device_id=(sp, blk), device_id_type=MESH,
            ).start()

        @pl.when(blk == tp)
        def _():
            att_all[:, mine] = att_own[rows, :]

    @scoped("attend")
    def attend(first, second):
        values = [attended(first), attended(second)]
        for blk, v in zip((first, second), values):
            att_own[pl.ds(pl.multiple_of(blk * BLK, BLK), BLK), :] = v
        for blk in (first, second):
            hand_out(blk)

    def inner(i, carry):
        attend(2 * i + 1, 2 * i + 2)
        return carry

    lax.fori_loop(0, 2, inner, 0)
    for to in (BP, BM):
        pass_on("u", (0, 0), to)
    lax.fori_loop(2, 3, inner, 0)
    arrive("kv")
    arrive("doc")
    docx[pl.ds(0, 8), :] = jnp.where(sp == 0, -1.0, doc_lr[pl.ds(0, 8), :].astype(F32))
    docx[pl.ds(16, 8), :] = jnp.where(sp == 15, -1.0, doc_lr[pl.ds(8, 8), :].astype(F32))

    def outer(i, carry):
        attend(i, i + 7)
        return carry

    lax.fori_loop(0, 1, outer, 0)

    @scoped("a2a_wait")
    def a2a_wait():
        local["ow"].wait()
        local["st"].wait()
        local["g1"].wait()
        arrive("a2a")

    a2a_wait()
    need("u", (3, 0))
    need("u", (1, 0))

    def project(n):
        cols = pl.ds(n * 512, 512)
        xbuf[:, cols] = dot(att_all[...], owv[:, cols]) + stv[:, cols].astype(F32)

    @scoped("projection")
    def projection():
        for n in range(4):
            project(n)

    projection()

    def cols_of(rank):
        dy, dz = ORDER[rank]
        return pl.ds(pl.multiple_of((((z + dz) % R) * R + (y + dy) % R) * BLK, BLK), BLK)

    HALF = BLK // 2
    half = lambda h: pl.ds(h * HALF, HALF)

    def fs_send(name, src, dst, i, dev, n=HALF):
        rows = pl.ds(i * n, n)
        to_partner = name[0] == "c"
        send(
            (name, i), fs.at[src[0], src[1], rows, :], fs.at[dst[0], dst[1], rows, :], dev,
            "c" if to_partner else name, fs.at[0] if to_partner else fs.at[0, 0],
            name if to_partner else None, fs.at[1, dst[1]] if to_partner else None,
        )

    @scoped("first_norm")
    def first_norm(h):
        centre, factor = moments(xbuf[half(h), :])
        for r in range(16):
            c = cols_of(r)
            v = (xbuf[half(h), c] - centre) * factor * g1[:, c]
            fs[0, 0, half(h), pl.ds(r * BLK, BLK)] = v.astype(BF16)

    for h in range(2):
        first_norm(h)
        if h == 0:
            fs_send("x_l", (0, 0), (0, 3), 0, right)
    fs_send("x_r", (0, 0), (0, 1), 1, left)
    fs_send("x_l", (0, 0), (0, 3), 1, right)
    fs_send("x_r", (0, 0), (0, 1), 0, left)
    for h in range(2):
        fs_send("c0", (0, 0), (1, 0), h, partner)

    @scoped("gather_rows")
    def gather_rows(name, h):
        arrive((name, h))
        if name == "x_2":
            fs_send("c2", (0, 2), (1, 2), h, partner, BLK // 4)
            return
        slot, onward, first = (3, right, 0) if name == "x_l" else (1, left, 1)
        if h == first:
            for q in (2 * h, 2 * h + 1):
                fs_send("x_2", (0, slot), (0, 2), q, onward, BLK // 4)
        fs_send(f"c{slot}", (0, slot), (1, slot), h, partner)

    def needs(w, ranks):
        for o in ranks:
            for origin in (o, (o[1], o[0])):
                if origin != (0, 0):
                    need(w, origin)

    @scoped("hidden_a")
    def hidden_a(dx):
        arrive(f"c{dx}")
        needs("u", ORDER[: KA // BLK])
        for n in range(HID // 256):
            cols = pl.ds(n * 256, 256)
            rows = fs[:, dx, :, 0:KA].reshape(2 * BLK, KA)
            hacc[min(dx, 2), :, cols] = dot(rows, up_all[0:KA, cols])

    @scoped("hidden")
    def hidden(dx):
        arrive(f"c{dx}")
        needs("u", ORDER)
        lo = 0 if dx == 2 else KA
        for n in range(HID // 256):
            cols = pl.ds(n * 256, 256)
            rows = fs[:, dx, :, lo:D].reshape(2 * BLK, D - lo)
            v = dot(rows, up_all[lo:D, cols])
            if lo:
                v = v + hacc[min(dx, 2), :, cols]
            v = jnp.maximum(v, 0.0)
            act[:, dx, :, cols] = (v * v).astype(BF16).reshape(2, BLK, 256)

    @scoped("product_a")
    def product_a(j):
        needs("d", ORDER[2 * j : 2 * j + 2])
        cols = pl.ds(j * CW, CW)
        for two in (pl.ds(0, 2), pl.ds(2, 2)):
            v = dot(act[1, two].reshape(2 * BLK, HID), dn_all[:, cols])
            psend[j, two] = v.astype(BF16).reshape(2, BLK, CW)
        send(("p", j), psend.at[j], prx.at[j], partner, "p", psend)

    @scoped("product_b")
    def product_b(j):
        cols = pl.ds(j * CW, CW)
        for two in (pl.ds(0, 2), pl.ds(2, 2)):
            pown[j, two] = dot(act[0, two].reshape(2 * BLK, HID), dn_all[:, cols]).reshape(2, BLK, CW)

    LO, HI = pl.ds(0, HALF), pl.ds(HALF, HALF)

    def pair(j, dx, rows=slice(None)):
        return pown[j, dx, rows, :] + prx[j, dx, rows, :].astype(F32)

    @scoped("pair_sum")
    def pair_sum(j):
        arrive(("p", j))
        s2[j] = pair(j, 2).astype(BF16)
        send("mid", s2.at[j, LO, :], mid.at[j, LO, :], right, "s2", s2, ("mid", j), mid.at[j])
        send("mid", s2.at[j, HI, :], mid.at[j, HI, :], left, "s2", s2, ("mid", j), mid.at[j])
        if j < 6:
            direct(j)
        macc[:, pl.ds(j * CW, CW)] = pair(j, 0)

    @scoped("direct")
    def direct(j):
        s1[j, HI, :] = pair(j, 1, HI).astype(BF16)
        s3[j, LO, :] = pair(j, 3, LO).astype(BF16)
        send("fin", s1.at[j, HI, :], fin.at[j, 0, HI, :], right, "s1", s1, ("fin", j), fin.at[j])
        send("fin", s3.at[j, LO, :], fin.at[j, 1, LO, :], left, "s3", s3, ("fin", j), fin.at[j])

    @scoped("middle")
    def middle(j):
        arrive(("mid", j))
        s1[j, LO, :] = (pair(j, 1, LO) + mid[j, LO, :].astype(F32)).astype(BF16)
        s3[j, HI, :] = (pair(j, 3, HI) + mid[j, HI, :].astype(F32)).astype(BF16)
        send("fin", s1.at[j, LO, :], fin.at[j, 0, LO, :], right, "s1", s1, ("fin", j), fin.at[j])
        send("fin", s3.at[j, HI, :], fin.at[j, 1, HI, :], left, "s3", s3, ("fin", j), fin.at[j])

    @scoped("total_sum")
    def total_sum(j):
        arrive(("fin", j))
        macc[:, pl.ds(j * CW, CW)] += fin[j, 0].astype(F32) + fin[j, 1].astype(F32)

    need("u", (0, 3))
    need("u", (0, 1))
    need("u", (2, 0))
    need("u", (3, 3))
    need("u", (3, 1))
    gather_rows("x_l", 0)
    gather_rows("x_r", 1)
    need("u", (1, 3))
    need("u", (1, 1))
    hidden_a(0)
    gather_rows("x_l", 1)
    gather_rows("x_r", 0)
    need("u", (2, 3))
    need("u", (2, 1))
    own_down(BP, BM)
    need("d", (3, 0))
    need("d", (1, 0))
    hidden_a(3)
    hidden_a(1)
    gather_rows("x_2", 0)
    gather_rows("x_2", 2)
    gather_rows("x_2", 1)
    gather_rows("x_2", 3)
    hidden(0)
    hidden(1)
    hidden(3)
    need("d", (0, 3))
    need("d", (0, 1))
    need("d", (2, 0))
    hidden(2)
    product_a(0)
    product_b(0)
    product_a(1)
    need("d", (3, 3))
    need("d", (3, 1))
    pair_sum(0)
    product_b(1)
    product_a(2)
    pair_sum(1)
    product_b(2)
    need("d", (1, 3))
    need("d", (1, 1))
    pair_sum(2)
    product_a(3)
    product_b(3)
    middle(0)
    product_a(4)
    pair_sum(3)
    middle(1)
    product_b(4)
    middle(2)
    pair_sum(4)
    need("d", (2, 3))
    need("d", (2, 1))
    product_a(5)
    middle(3)
    product_b(5)
    product_a(6)
    pair_sum(5)
    product_b(6)
    middle(4)
    product_a(7)
    pair_sum(6)
    product_b(7)
    pair_sum(7)
    middle(5)
    direct(6)
    direct(7)
    middle(6)
    total_sum(0)
    total_sum(1)
    total_sum(2)
    total_sum(3)
    total_sum(4)
    middle(7)
    total_sum(5)
    total_sum(6)
    total_sum(7)
    @scoped("last_norm")
    def last_norm(h):
        macc[half(h), :] += fs[0, 0, half(h), :].astype(F32)
        centre, factor = moments(macc[half(h), :])
        for r in range(16):
            c = cols_of(r)
            v = (macc[half(h), pl.ds(r * BLK, BLK)] - centre) * factor * g2[:, c]
            out[half(h), c] = v.astype(BF16)

    local["g2"].wait()
    for h in range(2):
        last_norm(h)

    @scoped("drain")
    def drain():
        for kind, key in ends:
            if kind == "s":
                wait(kind, key)

    drain()
    assert len(send_sems.index) == SENDS and len(recv_sems.index) == ARRIVALS


def far(v):
    return pltpu.with_memory_space_constraint(v, pltpu.HBM)


def per_device(q, kv, sink, doc, stream, ow, g1, up, dn, g2):
    vm, anyw = pl.BlockSpec(memory_space=pltpu.VMEM), pl.BlockSpec(memory_space=pl.ANY)
    smem = pl.BlockSpec(memory_space=pltpu.SMEM)
    return pl.pallas_call(
        kernel,
        out_shape=jax.ShapeDtypeStruct(stream.shape, BF16),
        in_specs=[anyw, anyw, smem, anyw, anyw, anyw, anyw, anyw, anyw, anyw],
        out_specs=vm,
        scratch_shapes=[
            pltpu.VMEM((1, D), F32),
            pltpu.VMEM((1, D), F32),
            pltpu.VMEM((1024, BLK), BF16),
            pltpu.VMEM((1024 + 2 * BLK, BLK), BF16),
            pltpu.VMEM((8, BLK), jnp.int32),
            pltpu.VMEM((16, BLK), jnp.int32),
            pltpu.VMEM((24, BLK), F32),
            pltpu.VMEM((BLK, D), BF16),
            pltpu.VMEM((1024, D), BF16),
            pltpu.VMEM((1024, BLK), BF16),
            pltpu.VMEM((BLK, 1024), BF16),
            pltpu.VMEM((BLK, D), F32),
            pltpu.VMEM((D, HID), BF16),
            pltpu.VMEM((HID, D), BF16),
            pltpu.VMEM((2, R, BLK, D), BF16),
            pltpu.VMEM((3, 2 * BLK, HID), F32),
            pltpu.VMEM((2, R, BLK, HID), BF16),
            pltpu.VMEM((NCH, R, BLK, CW), BF16),
            pltpu.VMEM((NCH, R, BLK, CW), BF16),
            pltpu.VMEM((NCH, R, BLK, CW), F32),
            pltpu.VMEM((NCH, BLK, CW), BF16),
            pltpu.VMEM((NCH, BLK, CW), BF16),
            pltpu.VMEM((NCH, BLK, CW), BF16),
            pltpu.VMEM((NCH, BLK, CW), BF16),
            pltpu.VMEM((NCH, 2, BLK, CW), BF16),
            pltpu.VMEM((BLK, D), F32),
            pltpu.SemaphoreType.DMA((SENDS,)),
            pltpu.SemaphoreType.DMA((ARRIVALS,)),
            pltpu.SemaphoreType.DMA((9,)),
        ],
        compiler_params=pltpu.CompilerParams(
            collective_id=0, has_side_effects=True, vmem_limit_bytes=48 * 1024 * 1024
        ),
        name="layer",
    )(
        far(q), far(kv.reshape(1024, BLK)), far(sink), far(doc.reshape(8, BLK)), far(stream), far(ow),
        far(g1.reshape(1, D)), far(up), far(dn), far(g2.reshape(1, D)),
    )


def solution(mesh):
    placed = (
        P("sp", "tp"),
        P("sp", "tp", None),
        P("tp"),
        P("sp"),
        P(("sp", "tp"), None),
        P(),
        P(),
        P("sp", "tp"),
        P("tp", "sp"),
        P(),
    )
    return jax.shard_map(
        per_device, mesh=mesh, in_specs=placed, out_specs=P(("sp", "tp"), None), check_vma=False
    )
```

```python
import functools

import jax
import jax.numpy as jnp
from jax import lax
from jax.experimental import pallas as pl
from jax.experimental.pallas import tpu as pltpu
from jax.sharding import PartitionSpec as P

MESH = pl.DeviceIdType.MESH
F32 = jnp.float32
BF16 = jnp.bfloat16
NEG_LARGE = -1e30
NORM_EPS = 1e-05
R = 4
BLK = 128
D = 2048
HID = 1024
NCH = 8
CW = D // NCH
SENDS, ARRIVALS = 13, 66

ORDER = [
    (0, 0), (1, 0), (3, 0), (0, 1), (0, 3), (3, 3), (3, 1), (1, 1),
    (1, 3), (2, 0), (0, 2), (3, 2), (2, 3), (2, 1), (1, 2), (2, 2),
]
RANK = {o: i for i, o in enumerate(ORDER)}

AP, AM, BP, BM = (1, 0), (-1, 0), (0, 1), (0, -1)
ONWARD = {
    (3, 0): [(AP, 0), (BP, None), (BM, None)],
    (1, 0): [(AM, 1), (BP, None), (BM, None)],
    (2, 0): [(BP, None), (BM, None)],
}
ONWARD |= {(da, 3): [(BP, 0)] for da in range(R)} | {(da, 1): [(BM, 1)] for da in range(R)}
TOGETHER = (((0, 2), (3, 2), (1, 2), (2, 2)),)
KA = HID


def nt_dot(a, b):
    return lax.dot_general(a, b, (((1,), (1,)), ((), ())), preferred_element_type=F32)


def dot(a, b):
    return jnp.dot(a, b, preferred_element_type=F32)


def moments(x):
    centre = jnp.mean(x, axis=-1, keepdims=True)
    shifted = x - centre
    return centre, lax.rsqrt(jnp.mean(shifted * shifted, axis=-1, keepdims=True) + NORM_EPS)


def scoped(name):
    def wrap(f):
        @functools.wraps(f)
        def run(*args):
            tag = "_".join("".join(c for c in str(v) if c.isalnum()) for v in args if isinstance(v, (int, str, tuple)))
            with jax.named_scope(f"{name}#v={tag}"):
                return f(*args)

        return run

    return wrap


class Sems:
    def __init__(self):
        self.index = {}

    def at(self, key):
        return self.index.setdefault(key, len(self.index))


def kernel(
    q_h, kv_h, sink_s, doc_h, st_h, ow_h, g1_h, up_h, dn_h, g2_h, out,
    g1, g2, qv, kvx, docv, doc_lr, docx, stv, owv, att_own, att_all, xbuf,
    up_all, dn_all, fs, hacc, act, psend, prx, pown, s1, s2, s3, mid, fin, macc,
    ss, rs, ls,
):
    sp, tp = lax.axis_index("sp"), lax.axis_index("tp")
    z, y = sp // R, sp % R
    x, core = tp // 2, tp % 2
    stride_a, stride_b = 1 + 3 * core, 4 - 3 * core
    a = y * (1 - core) + z * core
    b = z * (1 - core) + y * core

    def sp_of(da, db):
        return ((a + da) % R) * stride_a + ((b + db) % R) * stride_b

    partner = (sp, x * 2 + (1 - core))
    right = (sp, ((x + 1) % R) * 2 + core)
    left = (sp, ((x + R - 1) % R) * 2 + core)
    sp_next, sp_prev = (sp + 1) % 16, (sp + 15) % 16

    barrier = pltpu.get_barrier_semaphore()
    greet = [(sp, (tp + i) % 8) for i in range(1, 8)]
    greet += [(sp_of(da, db), tp) for da, db in ((1, 0), (3, 0), (0, 1), (0, 3))]
    greet += [(sp_next, tp), (sp_prev, tp)]
    for dev in greet:
        pl.semaphore_signal(barrier, inc=1, device_id=dev, device_id_type=MESH)
    local_names = ["kv", "doc", "up", "q", "st", "ow", "dn", "g1", "g2"]
    pairs = {
        "kv": (kv_h, kvx.at[pl.ds(BLK, 1024), :]),
        "doc": (doc_h, docv),
        "q": (q_h, qv),
        "up": (up_h, up_all.at[pl.ds(0, BLK), :]),
        "dn": (dn_h, dn_all.at[:, pl.ds(0, BLK)]),
        "st": (st_h, stv),
        "ow": (ow_h, owv),
        "g1": (g1_h, g1),
        "g2": (g2_h, g2),
    }
    local = {n: pltpu.make_async_copy(*pairs[n], ls.at[i]) for i, n in enumerate(local_names)}
    for n in local_names:
        local[n].start()

    pl.semaphore_wait(barrier, len(greet))

    send_sems, recv_sems = Sems(), Sems()
    ends = {}
    waited = set()

    def send(key, src, dst, dev, group, whole, with_key=None, with_dst=None):
        pltpu.make_async_remote_copy(
            src_ref=src, dst_ref=dst, send_sem=ss.at[send_sems.at(group)],
            recv_sem=rs.at[recv_sems.at(with_key or key)], device_id=dev, device_id_type=MESH,
        ).start()
        ends[("s", group)] = whole
        ends[("r", with_key or key)] = dst if with_dst is None else with_dst

    def wait(kind, key):
        ref = ends[(kind, key)]
        i = (send_sems if kind == "s" else recv_sems).at(key)
        copy = pltpu.make_async_remote_copy(
            src_ref=ref, dst_ref=ref, send_sem=ss.at[i], recv_sem=rs.at[i], device_id=partner, device_id_type=MESH
        )
        copy.wait_send() if kind == "s" else copy.wait_recv()

    def arrive(key):
        if key not in waited:
            waited.add(key)
            wait("r", key)

    local["kv"].wait()
    local["doc"].wait()
    rim = kvx.at[pl.ds(0, 2 * BLK), :]
    for src, dst, dev in ((1024, 0, sp_next), (BLK, 1024 + BLK, sp_prev)):
        rows = kvx.at[pl.ds(src, BLK), :], kvx.at[pl.ds(dst, BLK), :]
        send("kv", *rows, (dev, tp), "kv", rim, "kv", rim)
    send("doc", docv, doc_lr.at[pl.ds(0, 8), :], (sp_next, tp), "doc", doc_lr, "doc", doc_lr)
    send("doc", docv, doc_lr.at[pl.ds(8, 8), :], (sp_prev, tp), "doc", doc_lr, "doc", doc_lr)

    def block(w, origin, at, half):
        ra, rb = (origin[0] - at[0]) % R, (origin[1] - at[1]) % R
        r0, r1 = RANK[(ra, rb)], RANK[(rb, ra)]
        slot = (r0 + core * (r1 - r0)) * BLK
        size = BLK if w == "u" else HID
        lo, n = {None: (0, size), 0: (0, size // 2), 1: (size // 2, size // 2)}[half]
        if w == "u":
            return up_all.at[pl.ds(pl.multiple_of(slot + lo, BLK // 2), n), :]
        return dn_all.at[pl.ds(lo, n), pl.ds(pl.multiple_of(slot, BLK), BLK)]

    def pass_on(w, origin, to, half=None):
        rel = ((origin[0] - to[0]) % R, (origin[1] - to[1]) % R)
        held = up_all if w == "u" else dn_all
        together = {o: g for g in TOGETHER for o in g}.get(rel, (rel,)) if w == "u" else (rel,)
        n = len(together) * BLK
        send(
            (w, rel), block(w, origin, (0, 0), half), block(w, origin, to, half),
            (sp_of(to[0] % R, to[1] % R), tp),
            w, held.at[pl.ds(0, 15 * BLK), :] if w == "u" else held.at[:, pl.ds(0, 15 * BLK)],
            (w, together), held.at[pl.ds(0, n), :] if w == "u" else held.at[:, pl.ds(0, n)],
        )

    relayed = set()

    @scoped("need")
    def need(w, origin):
        if (w, origin) in relayed:
            return
        relayed.add((w, origin))
        arrive((w, {o: g for g in TOGETHER for o in g}.get(origin, (origin,)) if w == "u" else (origin,)))
        for to, h in ONWARD.get(origin, ()):
            pass_on(w, origin, to, h)

    def own_down(*ways):
        for to in ways:
            pass_on("d", (0, 0), to)

    local["up"].wait()
    for to in (AP, AM):
        pass_on("u", (0, 0), to)
    local["dn"].wait()
    own_down(AP, AM)

    local["q"].wait()
    docx[pl.ds(8, 8), :] = docv[...].astype(F32)
    row = lax.broadcasted_iota(jnp.int32, (BLK, BLK), 0)
    col = lax.broadcasted_iota(jnp.int32, (BLK, BLK), 1)
    low = col < 64
    a2a_send, a2a_recv = send_sems.at("a2a"), recv_sems.at("a2a")
    ends[("s", "a2a")] = ends[("r", "a2a")] = att_own.at[pl.ds(0, 7 * BLK), :]

    def attended(blk):
        rows = pl.ds(pl.multiple_of(blk * BLK, BLK), BLK)
        qf = qv[rows, :].astype(F32) * 0.125
        q2 = jnp.concatenate(
            [jnp.where(low, qf, 0.0), jnp.where(low, pltpu.roll(qf, 64, 1), 0.0)], axis=0
        ).astype(BF16)
        kvb = kvx[pl.ds(pl.multiple_of(blk * BLK, BLK), 3 * BLK), :]
        s = nt_dot(q2, kvb)
        dq = jnp.broadcast_to(docx[pl.ds(blk + 8, 1), :], (BLK, BLK)).T
        same = [jnp.broadcast_to(docx[pl.ds(blk + 7 + j, 1), :], (BLK, BLK)) == dq for j in range(3)]
        same[0] = same[0] & (col >= row)
        same[2] = same[2] & (col <= row)
        weights, scale = [], []
        for h in range(2):
            sink = sink_s[h]
            t = [
                jnp.where(same[j], s[h * BLK : (h + 1) * BLK, j * BLK : (j + 1) * BLK], NEG_LARGE)
                for j in range(3)
            ]
            top = jnp.max(jnp.maximum(jnp.maximum(t[0], t[1]), t[2]), axis=-1, keepdims=True)
            top = jnp.maximum(top, sink)
            p = [jnp.exp(v - top) for v in t]
            total = jnp.sum(p[0] + p[1] + p[2], axis=-1, keepdims=True) + jnp.exp(sink - top)
            weights.append(jnp.concatenate(p, axis=1).astype(BF16))
            scale.append(1.0 / total)
        o = dot(jnp.concatenate(weights, axis=0), kvb)
        o0, o1 = o[:BLK] * scale[0], o[BLK:] * scale[1]
        return jnp.where(low, pltpu.roll(o0, 64, 1), o1).astype(BF16)

    def hand_out(blk):
        rows = pl.ds(pl.multiple_of(blk * BLK, BLK), BLK)
        mine = pl.ds(pl.multiple_of(tp * BLK, BLK), BLK)

        @pl.when(blk != tp)
        def _():
            pltpu.make_async_remote_copy(
                src_ref=att_own.at[rows, :], dst_ref=att_all.at[:, mine],
                send_sem=ss.at[a2a_send], recv_sem=rs.at[a2a_recv],
                device_id=(sp, blk), device_id_type=MESH,
            ).start()

        @pl.when(blk == tp)
        def _():
            att_all[:, mine] = att_own[rows, :]

    @scoped("attend")
    def attend(first, second):
        values = [attended(first), attended(second)]
        for blk, v in zip((first, second), values):
            att_own[pl.ds(pl.multiple_of(blk * BLK, BLK), BLK), :] = v
        for blk in (first, second):
            hand_out(blk)

    def inner(i, carry):
        attend(2 * i + 1, 2 * i + 2)
        return carry

    lax.fori_loop(0, 2, inner, 0)
    for to in (BP, BM):
        pass_on("u", (0, 0), to)
    lax.fori_loop(2, 3, inner, 0)
    arrive("kv")
    arrive("doc")
    docx[pl.ds(0, 8), :] = jnp.where(sp == 0, -1.0, doc_lr[pl.ds(0, 8), :].astype(F32))
    docx[pl.ds(16, 8), :] = jnp.where(sp == 15, -1.0, doc_lr[pl.ds(8, 8), :].astype(F32))

    def outer(i, carry):
        attend(i, i + 7)
        return carry

    lax.fori_loop(0, 1, outer, 0)

    @scoped("a2a_wait")
    def a2a_wait():
        local["ow"].wait()
        local["st"].wait()
        local["g1"].wait()
        arrive("a2a")

    a2a_wait()
    need("u", (3, 0))
    need("u", (1, 0))

    def project(n):
        cols = pl.ds(n * 512, 512)
        xbuf[:, cols] = dot(att_all[...], owv[:, cols]) + stv[:, cols].astype(F32)

    @scoped("projection")
    def projection():
        for n in range(4):
            project(n)

    projection()

    def cols_of(rank):
        dy, dz = ORDER[rank]
        return pl.ds(pl.multiple_of((((z + dz) % R) * R + (y + dy) % R) * BLK, BLK), BLK)

    HALF = BLK // 2
    half = lambda h: pl.ds(h * HALF, HALF)

    def fs_send(name, src, dst, i, dev, n=HALF):
        rows = pl.ds(i * n, n)
        to_partner = name[0] == "c"
        send(
            (name, i), fs.at[src[0], src[1], rows, :], fs.at[dst[0], dst[1], rows, :], dev,
            "c" if to_partner else name, fs.at[0] if to_partner else fs.at[0, 0],
            name if to_partner else None, fs.at[1, dst[1]] if to_partner else None,
        )

    @scoped("first_norm")
    def first_norm(h):
        centre, factor = moments(xbuf[half(h), :])
        for r in range(16):
            c = cols_of(r)
            v = (xbuf[half(h), c] - centre) * factor * g1[:, c]
            fs[0, 0, half(h), pl.ds(r * BLK, BLK)] = v.astype(BF16)

    for h in range(2):
        first_norm(h)
        if h == 0:
            fs_send("x_l", (0, 0), (0, 3), 0, right)
    fs_send("x_r", (0, 0), (0, 1), 1, left)
    fs_send("x_l", (0, 0), (0, 3), 1, right)
    fs_send("x_r", (0, 0), (0, 1), 0, left)
    for h in range(2):
        fs_send("c0", (0, 0), (1, 0), h, partner)

    @scoped("gather_rows")
    def gather_rows(name, h):
        arrive((name, h))
        if name == "x_2":
            fs_send("c2", (0, 2), (1, 2), h, partner, BLK // 4)
            return
        slot, onward, first = (3, right, 0) if name == "x_l" else (1, left, 1)
        if h == first:
            for q in (2 * h, 2 * h + 1):
                fs_send("x_2", (0, slot), (0, 2), q, onward, BLK // 4)
        fs_send(f"c{slot}", (0, slot), (1, slot), h, partner)

    def needs(w, ranks):
        for o in ranks:
            for origin in (o, (o[1], o[0])):
                if origin != (0, 0):
                    need(w, origin)

    @scoped("hidden_a")
    def hidden_a(dx):
        arrive(f"c{dx}")
        needs("u", ORDER[: KA // BLK])
        for n in range(HID // 256):
            cols = pl.ds(n * 256, 256)
            rows = fs[:, dx, :, 0:KA].reshape(2 * BLK, KA)
            hacc[min(dx, 2), :, cols] = dot(rows, up_all[0:KA, cols])

    @scoped("hidden")
    def hidden(dx):
        arrive(f"c{dx}")
        needs("u", ORDER)
        lo = 0 if dx == 2 else KA
        for n in range(HID // 256):
            cols = pl.ds(n * 256, 256)
            rows = fs[:, dx, :, lo:D].reshape(2 * BLK, D - lo)
            v = dot(rows, up_all[lo:D, cols])
            if lo:
                v = v + hacc[min(dx, 2), :, cols]
            v = jnp.maximum(v, 0.0)
            act[:, dx, :, cols] = (v * v).astype(BF16).reshape(2, BLK, 256)

    @scoped("product_a")
    def product_a(j):
        needs("d", ORDER[2 * j : 2 * j + 2])
        cols = pl.ds(j * CW, CW)
        for two in (pl.ds(0, 2), pl.ds(2, 2)):
            v = dot(act[1, two].reshape(2 * BLK, HID), dn_all[:, cols])
            psend[j, two] = v.astype(BF16).reshape(2, BLK, CW)
            send("p", psend.at[j, two], prx.at[j, two], partner, "p", psend, ("p", j), prx.at[j])

    @scoped("product_b")
    def product_b(j):
        cols = pl.ds(j * CW, CW)
        for two in (pl.ds(0, 2), pl.ds(2, 2)):
            pown[j, two] = dot(act[0, two].reshape(2 * BLK, HID), dn_all[:, cols]).reshape(2, BLK, CW)

    LO, HI = pl.ds(0, HALF), pl.ds(HALF, HALF)

    def pair(j, dx, rows=slice(None)):
        return pown[j, dx, rows, :] + prx[j, dx, rows, :].astype(F32)

    @scoped("pair_sum")
    def pair_sum(j):
        arrive(("p", j))
        s2[j] = pair(j, 2).astype(BF16)
        send("mid", s2.at[j, LO, :], mid.at[j, LO, :], right, "s2", s2, ("mid", j), mid.at[j])
        send("mid", s2.at[j, HI, :], mid.at[j, HI, :], left, "s2", s2, ("mid", j), mid.at[j])
        if j < 6:
            direct(j)
        macc[:, pl.ds(j * CW, CW)] = pair(j, 0)

    @scoped("direct")
    def direct(j):
        s1[j, HI, :] = pair(j, 1, HI).astype(BF16)
        s3[j, LO, :] = pair(j, 3, LO).astype(BF16)
        send("fin", s1.at[j, HI, :], fin.at[j, 0, HI, :], right, "s1", s1, ("fin", j), fin.at[j])
        send("fin", s3.at[j, LO, :], fin.at[j, 1, LO, :], left, "s3", s3, ("fin", j), fin.at[j])

    @scoped("middle")
    def middle(j):
        arrive(("mid", j))
        s1[j, LO, :] = (pair(j, 1, LO) + mid[j, LO, :].astype(F32)).astype(BF16)
        s3[j, HI, :] = (pair(j, 3, HI) + mid[j, HI, :].astype(F32)).astype(BF16)
        send("fin", s1.at[j, LO, :], fin.at[j, 0, LO, :], right, "s1", s1, ("fin", j), fin.at[j])
        send("fin", s3.at[j, HI, :], fin.at[j, 1, HI, :], left, "s3", s3, ("fin", j), fin.at[j])

    @scoped("total_sum")
    def total_sum(j):
        arrive(("fin", j))
        macc[:, pl.ds(j * CW, CW)] += fin[j, 0].astype(F32) + fin[j, 1].astype(F32)

    need("u", (0, 3))
    need("u", (0, 1))
    need("u", (2, 0))
    need("u", (3, 3))
    need("u", (3, 1))
    gather_rows("x_l", 0)
    gather_rows("x_r", 1)
    need("u", (1, 3))
    need("u", (1, 1))
    hidden_a(0)
    gather_rows("x_l", 1)
    gather_rows("x_r", 0)
    need("u", (2, 3))
    need("u", (2, 1))
    own_down(BP, BM)
    need("d", (3, 0))
    need("d", (1, 0))
    hidden_a(3)
    hidden_a(1)
    gather_rows("x_2", 0)
    gather_rows("x_2", 2)
    gather_rows("x_2", 1)
    gather_rows("x_2", 3)
    hidden(0)
    hidden(1)
    hidden(3)
    hidden(2)
    need("d", (0, 3))
    need("d", (0, 1))
    product_a(0)
    need("d", (2, 0))
    product_b(0)
    product_a(1)
    need("d", (3, 3))
    need("d", (3, 1))
    pair_sum(0)
    product_b(1)
    product_a(2)
    pair_sum(1)
    product_b(2)
    need("d", (1, 3))
    need("d", (1, 1))
    pair_sum(2)
    product_a(3)
    product_b(3)
    middle(0)
    product_a(4)
    pair_sum(3)
    middle(1)
    product_b(4)
    middle(2)
    pair_sum(4)
    need("d", (2, 3))
    need("d", (2, 1))
    product_a(5)
    middle(3)
    product_b(5)
    product_a(6)
    pair_sum(5)
    product_b(6)
    middle(4)
    product_a(7)
    pair_sum(6)
    product_b(7)
    pair_sum(7)
    middle(5)
    direct(6)
    direct(7)
    middle(6)
    total_sum(0)
    total_sum(1)
    total_sum(2)
    total_sum(3)
    total_sum(4)
    middle(7)
    total_sum(5)
    total_sum(6)
    total_sum(7)
    @scoped("last_norm")
    def last_norm(h):
        macc[half(h), :] += fs[0, 0, half(h), :].astype(F32)
        centre, factor = moments(macc[half(h), :])
        for r in range(16):
            c = cols_of(r)
            v = (macc[half(h), pl.ds(r * BLK, BLK)] - centre) * factor * g2[:, c]
            out[half(h), c] = v.astype(BF16)

    local["g2"].wait()
    for h in range(2):
        last_norm(h)

    @scoped("drain")
    def drain():
        for kind, key in ends:
            if kind == "s":
                wait(kind, key)

    drain()
    assert len(send_sems.index) == SENDS and len(recv_sems.index) == ARRIVALS


def far(v):
    return pltpu.with_memory_space_constraint(v, pltpu.HBM)


def per_device(q, kv, sink, doc, stream, ow, g1, up, dn, g2):
    vm, anyw = pl.BlockSpec(memory_space=pltpu.VMEM), pl.BlockSpec(memory_space=pl.ANY)
    smem = pl.BlockSpec(memory_space=pltpu.SMEM)
    return pl.pallas_call(
        kernel,
        out_shape=jax.ShapeDtypeStruct(stream.shape, BF16),
        in_specs=[anyw, anyw, smem, anyw, anyw, anyw, anyw, anyw, anyw, anyw],
        out_specs=vm,
        scratch_shapes=[
            pltpu.VMEM((1, D), F32),
            pltpu.VMEM((1, D), F32),
            pltpu.VMEM((1024, BLK), BF16),
            pltpu.VMEM((1024 + 2 * BLK, BLK), BF16),
            pltpu.VMEM((8, BLK), jnp.int32),
            pltpu.VMEM((16, BLK), jnp.int32),
            pltpu.VMEM((24, BLK), F32),
            pltpu.VMEM((BLK, D), BF16),
            pltpu.VMEM((1024, D), BF16),
            pltpu.VMEM((1024, BLK), BF16),
            pltpu.VMEM((BLK, 1024), BF16),
            pltpu.VMEM((BLK, D), F32),
            pltpu.VMEM((D, HID), BF16),
            pltpu.VMEM((HID, D), BF16),
            pltpu.VMEM((2, R, BLK, D), BF16),
            pltpu.VMEM((3, 2 * BLK, HID), F32),
            pltpu.VMEM((2, R, BLK, HID), BF16),
            pltpu.VMEM((NCH, R, BLK, CW), BF16),
            pltpu.VMEM((NCH, R, BLK, CW), BF16),
            pltpu.VMEM((NCH, R, BLK, CW), F32),
            pltpu.VMEM((NCH, BLK, CW), BF16),
            pltpu.VMEM((NCH, BLK, CW), BF16),
            pltpu.VMEM((NCH, BLK, CW), BF16),
            pltpu.VMEM((NCH, BLK, CW), BF16),
            pltpu.VMEM((NCH, 2, BLK, CW), BF16),
            pltpu.VMEM((BLK, D), F32),
            pltpu.SemaphoreType.DMA((SENDS,)),
            pltpu.SemaphoreType.DMA((ARRIVALS,)),
            pltpu.SemaphoreType.DMA((9,)),
        ],
        compiler_params=pltpu.CompilerParams(
            collective_id=0, has_side_effects=True, vmem_limit_bytes=48 * 1024 * 1024
        ),
        name="layer",
    )(
        far(q), far(kv.reshape(1024, BLK)), far(sink), far(doc.reshape(8, BLK)), far(stream), far(ow),
        far(g1.reshape(1, D)), far(up), far(dn), far(g2.reshape(1, D)),
    )


def solution(mesh):
    placed = (
        P("sp", "tp"),
        P("sp", "tp", None),
        P("tp"),
        P("sp"),
        P(("sp", "tp"), None),
        P(),
        P(),
        P("sp", "tp"),
        P("tp", "sp"),
        P(),
    )
    return jax.shard_map(
        per_device, mesh=mesh, in_specs=placed, out_specs=P(("sp", "tp"), None), check_vma=False
    )
```
